128 devices in a mesh: st: 64 (over z, y, x), tp: 2 (over core).
Axes of the slice: x: 4, y: 4, z: 4, core: 2. Of those that a mesh axis runs over, the one named last changes fastest.
Arguments:
- hidden: bfloat16 [65536, 2048], P('st'), may hold values from -6 to 6
- norm_gain: float32 [2048], replicated, may hold values from 0.1 to 1.9
- store: bfloat16 [1536, 64, 2048], P('st'), may hold values from -6 to 6
- store_gain: float32 [2048], replicated, may hold values from 0.1 to 1.9
- passage_ids: int32 [512, 4], P('st'), may hold values from 0 to 1535, as said below
- w_pool: bfloat16 [2048, 1024], P(None, 'tp'), may hold values from -0.125 to 0.125
- pool_mix: bfloat16 [4, 256, 256], P('tp'), may hold values from -0.375 to 0.375
- w_branch: bfloat16 [1024, 2048], P('tp'), may hold values from -0.1875 to 0.1875
- w_query: bfloat16 [2048, 512], P(None, 'tp'), may hold values from -0.125 to 0.125
- w_key: bfloat16 [2048, 512], P(None, 'tp'), may hold values from -0.125 to 0.125
- w_value: bfloat16 [2048, 512], P(None, 'tp'), may hold values from -0.125 to 0.125
- sharpness: float32 [4], P('tp'), may hold values from 1 to 90
- w_out: bfloat16 [512, 2048], P('tp'), may hold values from -0.25 to 0.25
- w_gate: bfloat16 [2048, 2048], P(None, 'tp'), may hold values from -0.125 to 0.125
Outputs:
- mixed: bfloat16 [65536, 2048], P('st', 'tp')
The draws below stay inside these ranges and needn't reach their ends.
Inputs may be any that keep to these rules, and one draw needn't show every extreme that they name: `passage_ids`: passage p lies on index p // 24 of st. The ids of one sequence's blocks (aligned rows of 32 ids) name passages of at most 1 reads on any one holder, counted with repeats, and some sequence reaches 1 at some holder in every draw.
All inputs are finite; a program needn't handle non-finite values.
Results may differ from the reference program's by a relative error of at most 0.0095.
The reference program's roundings to bfloat16 on the way (of `normed`, `pool_in`, `pooled`, `pool_out`, `query`, `passage_normed`, `weights` and `read`) count: a program that leaves them out, or rounds other values in their place, can miss the bound.
Values may be sent and summed in bfloat16 or wider, within the bound.
No kernel may reach another device: no remote copies, remote signals or barrier semaphores. Data moves between devices by JAX's collectives and lax.ppermute only.
A program may use at most 128 MiB of HBM per device.

```python
import jax
import jax.numpy as jnp
from jax import lax

D = 2048
GROUPS = 4
GROUP_DIM = 256
XHEADS = 4
HEAD_DIM = 128
BLOCK = 128
PER_BLOCK = 4
PLEN = 64
PASS_DEV = 24
TOK_DEV = 1024
POOL_WIDTH = 1024
XWIDTH = 512
TOKENS = 65536
BLOCKS = 512
REQ_DEV = 32
MOST = 1
PASSAGES = 1536
N_ST = 64
N_TP = 2


def draw_passage_ids(key, part):
    keys = jax.random.split(jax.random.fold_in(key, 11), 5)
    slots = N_ST * MOST
    devices = jnp.arange(N_ST)[:, None]
    slot_owner = jnp.broadcast_to(jnp.arange(slots)[None, :] // MOST, (N_ST, slots))
    forced = (slot_owner == (devices - 1) % N_ST) | (slot_owner == (devices + N_ST // 2) % N_ST)
    noise = jax.random.randint(keys[0], (N_ST, slots), 0, 1 << 20)
    score = jnp.where(forced, 0, noise + 1) * slots + jnp.arange(slots)[None, :]
    order = jnp.argsort(score, axis=1)[:, :REQ_DEV]
    chosen = jnp.take_along_axis(slot_owner, order, axis=1)
    shuffle = jax.random.randint(keys[1], (N_ST, REQ_DEV), 0, 1 << 20) * REQ_DEV + jnp.arange(REQ_DEV)[None, :]
    owners = jnp.take_along_axis(chosen, jnp.argsort(shuffle, axis=1), axis=1)
    local = jnp.minimum(jax.random.randint(keys[2], (N_ST, REQ_DEV), 0, PASS_DEV), jax.random.randint(keys[3], (N_ST, REQ_DEV), 0, PASS_DEV))
    local = jnp.minimum(local, jax.random.randint(keys[4], (N_ST, REQ_DEV), 0, PASS_DEV))
    return (owners * PASS_DEV + local).reshape(BLOCKS, PER_BLOCK).astype(jnp.int32)


def draw_sharpness(key, part):
    spread = jax.random.uniform(jax.random.fold_in(key, 23), (XHEADS,), jnp.float32)
    return jnp.exp(jnp.log(1.0) + spread * (jnp.log(4.0) - jnp.log(1.0)))


def steps_of(key, extent, cuts, low, largest):
    level, own = 1.0, jax.random.fold_in(key, 6)
    for dim, blocks in cuts:
        draws = jnp.exp(jax.random.uniform(jax.random.fold_in(own, dim), (blocks,), jnp.float32, low / len(cuts), largest / len(cuts)))
        level = level * jnp.repeat(draws, extent[dim] // blocks).reshape([-1 if axis == dim else 1 for axis in range(len(extent))])
    return level


def scatter_about(rng, extent, scale, reach, cuts=(), held_as=jnp.bfloat16):
    drawn = scale * jax.random.normal(rng, extent, jnp.float32)
    if cuts:
        drawn = drawn * steps_of(rng, extent, cuts, -0.22, 0.18)
    return jnp.clip(drawn, -reach, reach).astype(held_as)


def setup_inputs(seed: int = 0) -> dict:
    streams_of = jax.random.split(jax.random.key(seed), 15)
    hidden = scatter_about(streams_of[0], (TOKENS, D), 1.0, 6.0, ((0, 64),))
    norm_gain = jnp.clip(1.0 + 0.18 * jax.random.normal(streams_of[1], (D,), jnp.float32), 0.1, 1.9)
    store = scatter_about(streams_of[2], (PASSAGES, PLEN, D), 1.0, 6.0, ((0, 64),))
    store_gain = jnp.clip(1.0 + 0.18 * jax.random.normal(streams_of[3], (D,), jnp.float32), 0.1, 1.9)
    passage_ids = draw_passage_ids(jax.random.fold_in(streams_of[14], 71), 0)
    w_pool = scatter_about(streams_of[5], (D, POOL_WIDTH), D ** -0.5, 0.125, ((1, 2),))
    pool_mix = scatter_about(streams_of[6], (GROUPS, GROUP_DIM, GROUP_DIM), GROUP_DIM ** -0.5, 0.375, ((0, 2),))
    w_branch = scatter_about(streams_of[7], (POOL_WIDTH, D), POOL_WIDTH ** -0.5, 0.1875, ((0, 2),))
    w_query = scatter_about(streams_of[8], (D, XWIDTH), D ** -0.5, 0.125, ((1, 2),))
    w_key = scatter_about(streams_of[9], (D, XWIDTH), D ** -0.5, 0.125, ((1, 2),))
    w_value = scatter_about(streams_of[10], (D, XWIDTH), D ** -0.5, 0.125, ((1, 2),))
    sharpness = draw_sharpness(jax.random.fold_in(streams_of[14], 71), 0)
    w_out = scatter_about(streams_of[12], (XWIDTH, D), XWIDTH ** -0.5, 0.25, ((0, 2),))
    w_gate = scatter_about(streams_of[13], (D, D), D ** -0.5, 0.125, ((1, 2),))
    return {"hidden": hidden, "norm_gain": norm_gain, "store": store, "store_gain": store_gain, "passage_ids": passage_ids, "w_pool": w_pool, "pool_mix": pool_mix, "w_branch": w_branch, "w_query": w_query, "w_key": w_key, "w_value": w_value, "sharpness": sharpness, "w_out": w_out, "w_gate": w_gate}


def rms_norm(values, gain):
    wide = values.astype(jnp.float32)
    scale = lax.rsqrt(lax.optimization_barrier(jnp.mean(wide * wide, axis=-1, keepdims=True)) + 1e-05)
    return wide * scale * gain

def split_sum(left, right, pieces):
    width = left.shape[1] // pieces
    total = jnp.zeros((left.shape[0], right.shape[1]), jnp.float32)
    for index in range(pieces):
        term = jnp.dot(left[:, index * width:(index + 1) * width], right[index * width:(index + 1) * width], preferred_element_type=jnp.float32).astype(jnp.bfloat16)
        term = lax.optimization_barrier(term)
        total = total + term.astype(jnp.float32)
    return total

def reference(hidden, norm_gain, store, store_gain, passage_ids, w_pool, pool_mix, w_branch, w_query, w_key, w_value, sharpness, w_out, w_gate):
    normed = rms_norm(hidden, norm_gain).astype(jnp.bfloat16)
    pool_in = jnp.dot(normed, w_pool, preferred_element_type=jnp.float32).astype(jnp.bfloat16)
    grouped = pool_in.astype(jnp.float32).reshape(N_ST, TOK_DEV, GROUPS, GROUP_DIM)
    position = jnp.arange(TOK_DEV)
    outputs = []
    for group in range(GROUPS):
        window = 2 ** (group + 1)
        column = grouped[:, :, group]
        total = jnp.zeros_like(column)
        for shift in range(window):
            total = total + jnp.pad(column, ((0, 0), (shift, 0), (0, 0)))[:, :TOK_DEV]
        count = jnp.minimum(position + 1, window).astype(jnp.float32)[None, :, None]
        outputs.append(total / count - column)
    pooled = jnp.stack(outputs, axis=2).astype(jnp.bfloat16)
    pool_out = jnp.einsum('ntgc,gcd->ntgd', pooled.astype(jnp.float32), pool_mix.astype(jnp.float32))
    pool_out = pool_out.astype(jnp.bfloat16).reshape(TOKENS, POOL_WIDTH)
    branch_pool = split_sum(pool_out, w_branch, N_TP)
    query = jnp.dot(normed, w_query, preferred_element_type=jnp.float32).astype(jnp.bfloat16)
    query_blocks = query.reshape(BLOCKS, BLOCK, XHEADS, HEAD_DIM)
    scale = sharpness / HEAD_DIM ** 0.5

    def one_block(items):
        block_query, ids = items
        rows = store[ids].reshape(PER_BLOCK * PLEN, D)
        passage_normed = rms_norm(rows, store_gain).astype(jnp.bfloat16)
        keys = jnp.dot(passage_normed, w_key, preferred_element_type=jnp.float32).astype(jnp.bfloat16)
        values = jnp.dot(passage_normed, w_value, preferred_element_type=jnp.float32).astype(jnp.bfloat16)
        keys = keys.reshape(PER_BLOCK * PLEN, XHEADS, HEAD_DIM).astype(jnp.float32)
        values = values.reshape(PER_BLOCK * PLEN, XHEADS, HEAD_DIM).astype(jnp.float32)
        scores = jnp.einsum('qhd,khd->hqk', block_query.astype(jnp.float32), keys) * scale[:, None, None]
        weights = jax.nn.softmax(scores, axis=-1).astype(jnp.bfloat16)
        read = jnp.einsum('hqk,khd->qhd', weights.astype(jnp.float32), values)
        return read.astype(jnp.bfloat16).reshape(BLOCK, XWIDTH)
    read = lax.map(one_block, (query_blocks, passage_ids)).reshape(TOKENS, XWIDTH)
    branch_read = split_sum(read, w_out, N_TP)
    gate = jax.nn.sigmoid(jnp.dot(normed, w_gate, preferred_element_type=jnp.float32))
    return (branch_pool + gate * branch_read).astype(jnp.bfloat16)
```

```python
import functools
import math

import jax
import jax.numpy as jnp
from jax import lax
from jax.experimental import pallas as pl
from jax.experimental.pallas import tpu as pltpu
from jax.sharding import PartitionSpec as P

F32, BF16 = jnp.float32, jnp.bfloat16
EPS = 1e-05
CARRY = 16
SWAP = [(0, 1), (1, 0)]


def rms_norm(wide, gain):
    scale = lax.rsqrt(jnp.mean(wide * wide, axis=-1, keepdims=True) + EPS)
    return (wide * scale * gain).astype(BF16)


def dot(a, b):
    return jnp.dot(a, b, preferred_element_type=F32)


def cost(flops, bytes_accessed, transcendentals=0):
    return pl.CostEstimate(
        flops=flops, bytes_accessed=bytes_accessed, transcendentals=transcendentals
    )


def params(mib, **kw):
    return pltpu.CompilerParams(vmem_limit_bytes=mib << 20, **kw)


def project_kernel(rows_ref, gain_ref, key_ref, value_ref, out_ref):
    normed = rms_norm(rows_ref[...].astype(F32), gain_ref[...])
    width = key_ref.shape[1]
    out_ref[:, :width] = dot(normed, key_ref[...]).astype(BF16)
    out_ref[:, width:] = dot(normed, value_ref[...]).astype(BF16)


def project(store, gain, w_key, w_value):
    count, length, width = store.shape
    rows = count * length
    tile = 256
    kv = w_key.shape[1] + w_value.shape[1]
    return pl.pallas_call(
        project_kernel,
        grid=(rows // tile,),
        in_specs=[
            pl.BlockSpec((tile, width), lambda i: (i, 0)),
            pl.BlockSpec((1, width), lambda i: (0, 0)),
            pl.BlockSpec(w_key.shape, lambda i: (0, 0)),
            pl.BlockSpec(w_value.shape, lambda i: (0, 0)),
        ],
        out_specs=pl.BlockSpec((tile, kv), lambda i: (i, 0)),
        out_shape=jax.ShapeDtypeStruct((rows, kv), BF16),
        compiler_params=params(24),
        cost_estimate=cost(2 * rows * width * kv, rows * (width + kv) * 2 + width * kv * 2),
        name="project",
    )(store.reshape(rows, width), gain.reshape(1, width), w_key, w_value)


def place_kernel(request_ref, kv_ref, out_ref, sems):
    readers = out_ref.shape[0]

    def copy(r):
        which = jnp.maximum(request_ref[r] - 1, 0)
        return pltpu.make_async_copy(kv_ref.at[which], out_ref.at[r], sems.at[r])

    def start(r, _):
        @pl.when(request_ref[r] > 0)
        def _():
            copy(r).start()

        return 0

    def finish(r, _):
        @pl.when(request_ref[r] > 0)
        def _():
            copy(r).wait()

        return 0

    lax.fori_loop(0, readers, start, 0)
    lax.fori_loop(0, readers, finish, 0)


def place(request, kv):
    readers = request.shape[0]
    return pl.pallas_call(
        place_kernel,
        in_specs=[
            pl.BlockSpec(memory_space=pltpu.SMEM),
            pl.BlockSpec(memory_space=pltpu.VMEM),
        ],
        out_specs=pl.BlockSpec(memory_space=pl.ANY),
        out_shape=jax.ShapeDtypeStruct((readers,) + kv.shape[1:], BF16),
        scratch_shapes=[pltpu.SemaphoreType.DMA((readers,))],
        compiler_params=params(8),
        cost_estimate=cost(0, 6 << 20),
        name="place",
    )(request, kv)


def front_kernel(
    half_ref, hidden_ref, gain_ref, pool_ref, query_ref, gate_ref, mix_ref,
    pool_out_ref, query_out_ref, gate_out_ref, carry,
):
    step = pl.program_id(0)
    tile = hidden_ref.shape[0]
    groups, dim = mix_ref.shape[0], mix_ref.shape[1]

    @pl.when(step == 0)
    def _():
        carry[...] = jnp.zeros_like(carry)

    normed = rms_norm(hidden_ref[...].astype(F32), gain_ref[...])
    pool_in = dot(normed, pool_ref[...]).astype(BF16)
    query_out_ref[...] = dot(normed, query_ref[...]).astype(BF16)
    gate_out_ref[...] = jax.nn.sigmoid(dot(normed, gate_ref[...]))
    recent = jnp.concatenate([carry[...], pool_in], axis=0)
    carry[...] = pool_in[tile - CARRY :]
    shape = (tile, tile + CARRY)
    back = (
        lax.broadcasted_iota(jnp.int32, shape, 0)
        + CARRY
        - lax.broadcasted_iota(jnp.int32, shape, 1)
    )
    position = step * tile + lax.broadcasted_iota(jnp.int32, (tile, 1), 0)
    for g in range(groups):
        window = jnp.left_shift(2, half_ref[0] * groups + g)
        band = jnp.where((back >= 0) & (back < window), 1.0, 0.0).astype(BF16)
        columns = slice(g * dim, (g + 1) * dim)
        total = dot(band, recent[:, columns])
        count = jnp.minimum(position + 1, window).astype(F32)
        pooled = (total / count - pool_in[:, columns].astype(F32)).astype(BF16)
        pool_out_ref[:, columns] = dot(pooled, mix_ref[g]).astype(BF16)


def front(half, hidden, gain, w_pool, w_query, w_gate, pool_mix):
    tokens, width = hidden.shape
    tile = 256
    fixed = lambda a: pl.BlockSpec(a.shape, lambda i: (0,) * a.ndim)
    rowed = lambda n: pl.BlockSpec((tile, n), lambda i: (i, 0))
    gain = gain.reshape(1, width)
    outs = (w_pool.shape[1], w_query.shape[1], w_gate.shape[1])
    return pl.pallas_call(
        front_kernel,
        grid=(tokens // tile,),
        in_specs=[
            pl.BlockSpec(memory_space=pltpu.SMEM),
            rowed(width),
            fixed(gain),
            fixed(w_pool),
            fixed(w_query),
            fixed(w_gate),
            fixed(pool_mix),
        ],
        out_specs=[rowed(n) for n in outs],
        out_shape=[
            jax.ShapeDtypeStruct((tokens, outs[0]), BF16),
            jax.ShapeDtypeStruct((tokens, outs[1]), BF16),
            jax.ShapeDtypeStruct((tokens, outs[2]), F32),
        ],
        scratch_shapes=[pltpu.VMEM((CARRY, outs[0]), BF16)],
        compiler_params=params(40),
        cost_estimate=cost(2 * tokens * width * sum(outs), 24 << 20, tokens * outs[2]),
        name="front",
    )(half, hidden, gain, w_pool, w_query, w_gate, pool_mix)


def branch_kernel(own_ref, other_ref, w_own_ref, w_other_ref, out_ref):
    own = dot(own_ref[...], w_own_ref[...]).astype(BF16).astype(F32)
    out_ref[...] = own + dot(other_ref[...], w_other_ref[...]).astype(BF16).astype(F32)


def branch(own, other, w_own, w_other):
    tokens, depth = own.shape
    width = w_own.shape[1]
    tile = 256
    return pl.pallas_call(
        branch_kernel,
        grid=(tokens // tile,),
        in_specs=[
            pl.BlockSpec((tile, depth), lambda i: (i, 0)),
            pl.BlockSpec((tile, depth), lambda i: (i, 0)),
            pl.BlockSpec((depth, width), lambda i: (0, 0)),
            pl.BlockSpec((depth, width), lambda i: (0, 0)),
        ],
        out_specs=pl.BlockSpec((tile, width), lambda i: (i, 0)),
        out_shape=jax.ShapeDtypeStruct((tokens, width), F32),
        compiler_params=params(24),
        cost_estimate=cost(4 * tokens * depth * width, 8 << 20),
        name="branch",
    )(own, other, w_own, w_other)


def attend_kernel(slot_ref, sharp_ref, query_ref, kv_ref, out_ref, held, sems, *, reads):
    count, length, width = held.shape[0], held.shape[1], held.shape[2]
    heads = sharp_ref.shape[0]
    half = width // 2
    dim = half // heads
    blocks = count // reads
    block = query_ref.shape[0] // blocks

    def copy(r):
        return pltpu.make_async_copy(kv_ref.at[slot_ref[r]], held.at[r], sems.at[r])

    for r in range(count):
        copy(r).start()

    def one_block(b, _):
        for j in range(reads):
            copy(b * reads + j).wait()
        rows = pl.ds(pl.multiple_of(b * block, block), block)
        memory = held[pl.ds(b * reads, reads)].reshape(reads * length, width)
        query = query_ref[rows, :]
        for h in range(heads):
            keys = memory[:, h * dim : (h + 1) * dim]
            values = memory[:, half + h * dim : half + (h + 1) * dim]
            scores = lax.dot_general(
                query[:, h * dim : (h + 1) * dim], keys, (((1,), (1,)), ((), ())),
                preferred_element_type=F32,
            )
            scores = scores * (sharp_ref[h] / math.sqrt(dim))
            scores = jnp.exp(scores - jnp.max(scores, axis=-1, keepdims=True))
            weights = (scores / jnp.sum(scores, axis=-1, keepdims=True)).astype(BF16)
            out_ref[rows, h * dim : (h + 1) * dim] = dot(weights, values).astype(BF16)
        return 0

    lax.fori_loop(0, blocks, one_block, 0)


def attend(slots, sharpness, query, kv, reads):
    count = slots.shape[0]
    return pl.pallas_call(
        functools.partial(attend_kernel, reads=reads),
        in_specs=[
            pl.BlockSpec(memory_space=pltpu.SMEM),
            pl.BlockSpec(memory_space=pltpu.SMEM),
            pl.BlockSpec(memory_space=pltpu.VMEM),
            pl.BlockSpec(memory_space=pl.ANY),
        ],
        out_specs=pl.BlockSpec(memory_space=pltpu.VMEM),
        out_shape=jax.ShapeDtypeStruct(query.shape, BF16),
        scratch_shapes=[
            pltpu.VMEM((count,) + kv.shape[1:], BF16),
            pltpu.SemaphoreType.DMA((count,)),
        ],
        compiler_params=params(16),
        cost_estimate=cost(1 << 30, 3 << 20, 1 << 19),
        name="attend",
    )(slots, sharpness, query, kv)


def mixed_kernel(own_ref, other_ref, w_own_ref, w_other_ref, pool_ref, gate_ref, out_ref):
    own = dot(own_ref[...], w_own_ref[...]).astype(BF16).astype(F32)
    read = own + dot(other_ref[...], w_other_ref[...]).astype(BF16).astype(F32)
    out_ref[...] = (pool_ref[...] + gate_ref[...] * read).astype(BF16)


def mix(own, other, w_own, w_other, pool, gate):
    tokens, depth = own.shape
    width = w_own.shape[1]
    tile = 256
    rowed = lambda n: pl.BlockSpec((tile, n), lambda i: (i, 0))
    fixed = pl.BlockSpec((depth, width), lambda i: (0, 0))
    return pl.pallas_call(
        mixed_kernel,
        grid=(tokens // tile,),
        in_specs=[rowed(depth), rowed(depth), fixed, fixed, rowed(width), rowed(width)],
        out_specs=rowed(width),
        out_shape=jax.ShapeDtypeStruct((tokens, width), BF16),
        compiler_params=params(24),
        cost_estimate=cost(4 * tokens * depth * width, 12 << 20),
        name="mixed",
    )(own, other, w_own, w_other, pool, gate)


def body(
    hidden, norm_gain, store, store_gain, passage_ids, w_pool, pool_mix, w_branch,
    w_query, w_key, w_value, sharpness, w_out, w_gate,
):
    half = lax.axis_index("tp")
    holders = lax.axis_size("st")
    count, length, _ = store.shape
    reads = passage_ids.shape[1]
    flat = passage_ids.reshape(-1)
    owner, local = flat // count, flat % count
    hits = owner[None, :] == jnp.arange(holders, dtype=jnp.int32)[:, None]
    request = jnp.sum(jnp.where(hits, local[None, :] + 1, 0), axis=1).reshape(holders, 1, 1)
    incoming = lax.all_to_all(request, "st", split_axis=0, concat_axis=0, tiled=True)
    kv = project(store, store_gain, w_key, w_value).reshape(count, length, -1)
    sent = place(incoming.reshape(-1), kv)
    arrived = lax.all_to_all(sent, "st", split_axis=0, concat_axis=0, tiled=True)

    columns = w_branch.shape[1] // 2

    def weights(w):
        mine = lax.dynamic_slice_in_dim(w, half * columns, columns, axis=1)
        theirs = lax.dynamic_slice_in_dim(w, (1 - half) * columns, columns, axis=1)
        return mine, lax.ppermute(theirs, "tp", SWAP)

    branch_own, branch_other = weights(w_branch)
    out_own, out_other = weights(w_out)
    pool_out, query, gate = front(
        half.reshape(1), hidden, norm_gain, w_pool, w_query, w_gate, pool_mix
    )
    pool = branch(pool_out, lax.ppermute(pool_out, "tp", SWAP), branch_own, branch_other)
    read = attend(owner, sharpness, query, arrived, reads)
    return mix(read, lax.ppermute(read, "tp", SWAP), out_own, out_other, pool, gate)


def solution(mesh):
    placed = (
        P("st", None), P(), P("st", None, None), P(), P("st", None), P(None, "tp"),
        P("tp", None, None), P("tp", None), P(None, "tp"), P(None, "tp"), P(None, "tp"),
        P("tp"), P("tp", None), P(None, "tp"),
    )
    return jax.shard_map(body, mesh=mesh, in_specs=placed, out_specs=P("st", "tp"), check_vma=False)
```

```python
import functools
import math

import jax
import jax.numpy as jnp
from jax import lax
from jax.experimental import pallas as pl
from jax.experimental.pallas import tpu as pltpu
from jax.sharding import PartitionSpec as P

F32, BF16 = jnp.float32, jnp.bfloat16
EPS = 1e-05
CARRY = 16
AHEAD = 3
SWAP = [(0, 1), (1, 0)]


def rms_norm(wide, gain):
    scale = lax.rsqrt(jnp.mean(wide * wide, axis=-1, keepdims=True) + EPS)
    return (wide * scale * gain).astype(BF16)


def dot(a, b):
    return jnp.dot(a, b, preferred_element_type=F32)


def cost(flops, bytes_accessed, transcendentals=0):
    return pl.CostEstimate(
        flops=flops, bytes_accessed=bytes_accessed, transcendentals=transcendentals
    )


def params(mib, **kw):
    return pltpu.CompilerParams(vmem_limit_bytes=mib << 20, **kw)


def owner_of(p, count):
    return lax.shift_right_logical(p * (-(-(1 << 20) // count)), 20)


def request_kernel(ids_ref, out_ref, *, count):
    holder = lax.broadcasted_iota(jnp.int32, (out_ref.shape[0], out_ref.shape[2]), 0)
    row = jnp.zeros_like(holder)
    for j in range(ids_ref.shape[0]):
        for b in range(ids_ref.shape[1]):
            p = ids_ref[j, b]
            owner = owner_of(p, count)
            row = jnp.where(holder == owner, p - owner * count + 1, row)
    out_ref[...] = row.reshape(out_ref.shape)


def requests(ids, count, holders):
    return pl.pallas_call(
        functools.partial(request_kernel, count=count),
        in_specs=[pl.BlockSpec(memory_space=pltpu.SMEM)],
        out_specs=pl.BlockSpec(memory_space=pltpu.VMEM),
        out_shape=jax.ShapeDtypeStruct((holders, 1, 128), jnp.int32),
        name="requests",
    )(ids)


def offer_kernel(
    asked_ref, store_ref, gain_ref, key_ref, value_ref, out_ref, rows, held, in_sems, out_sems
):
    count, length, width = rows.shape
    tiles = in_sems.shape[0]
    per = count // tiles
    tile = per * length
    half = key_ref.shape[1]

    def load(i):
        part = pl.ds(i * per, per)
        return pltpu.make_async_copy(store_ref.at[part], rows.at[part], in_sems.at[i])

    for i in range(min(AHEAD, tiles)):
        load(i).start()
    for i in range(tiles):
        load(i).wait()
        if i + AHEAD < tiles:
            load(i + AHEAD).start()
        part = slice(i * per, (i + 1) * per)
        normed = rms_norm(rows[part].reshape(tile, width).astype(F32), gain_ref[...])
        held[part, :, :half] = dot(normed, key_ref[...]).astype(BF16).reshape(per, length, half)
        held[part, :, half:] = dot(normed, value_ref[...]).astype(BF16).reshape(per, length, half)
    readers = out_ref.shape[0]
    asked = [asked_ref[r, 0, 0] for r in range(readers)]
    copies = [
        pltpu.make_async_copy(held.at[jnp.maximum(asked[r] - 1, 0)], out_ref.at[r], out_sems.at[r])
        for r in range(readers)
    ]
    for r in range(readers):
        pl.when(asked[r] > 0)(copies[r].start)
    for r in range(readers):
        pl.when(asked[r] > 0)(copies[r].wait)


def offer(asked, store, gain, w_key, w_value):
    count, length, width = store.shape
    readers, tiles, n = asked.shape[0], 6, 2 * w_key.shape[1]
    return pl.pallas_call(
        offer_kernel,
        in_specs=[
            pl.BlockSpec(memory_space=pltpu.SMEM),
            pl.BlockSpec(memory_space=pl.ANY),
            pl.BlockSpec(memory_space=pltpu.VMEM),
            pl.BlockSpec(memory_space=pltpu.VMEM),
            pl.BlockSpec(memory_space=pltpu.VMEM),
        ],
        out_specs=pl.BlockSpec(memory_space=pl.ANY),
        out_shape=jax.ShapeDtypeStruct((readers, length, n), BF16),
        scratch_shapes=[
            pltpu.VMEM(store.shape, BF16),
            pltpu.VMEM((count, length, n), BF16),
            pltpu.SemaphoreType.DMA((tiles,)),
            pltpu.SemaphoreType.DMA((readers,)),
        ],
        compiler_params=params(60),
        cost_estimate=cost(2 * count * length * width * n, 9 << 20),
        name="offer",
    )(asked, store, gain.reshape(1, width), w_key, w_value)


def front_kernel(
    half_ref, hidden_ref, gain_ref, pool_ref, query_ref, gate_ref, mix_ref,
    pool_out_ref, query_out_ref, gate_out_ref, carry,
):
    step = pl.program_id(0)
    tile = hidden_ref.shape[0]
    groups, dim = mix_ref.shape[0], mix_ref.shape[1]

    @pl.when(step == 0)
    def _():
        carry[...] = jnp.zeros_like(carry)

    normed = rms_norm(hidden_ref[...].astype(F32), gain_ref[...])
    pool_in = dot(normed, pool_ref[...]).astype(BF16)
    query_out_ref[...] = dot(normed, query_ref[...]).astype(BF16)
    gate_out_ref[...] = jax.nn.sigmoid(dot(normed, gate_ref[...])).astype(BF16)
    recent = jnp.concatenate([carry[...], pool_in], axis=0)
    carry[...] = pool_in[tile - CARRY :]
    shape = (tile, tile + CARRY)
    back = (
        lax.broadcasted_iota(jnp.int32, shape, 0)
        + CARRY
        - lax.broadcasted_iota(jnp.int32, shape, 1)
    )
    position = step * tile + lax.broadcasted_iota(jnp.int32, (tile, 1), 0)
    for g in range(groups):
        window = jnp.left_shift(2, half_ref[0] * groups + g)
        band = jnp.where((back >= 0) & (back < window), 1.0, 0.0).astype(BF16)
        columns = slice(g * dim, (g + 1) * dim)
        total = dot(band, recent[:, columns])
        count = jnp.minimum(position + 1, window).astype(F32)
        pooled = (total / count - pool_in[:, columns].astype(F32)).astype(BF16)
        pool_out_ref[:, columns] = dot(pooled, mix_ref[g]).astype(BF16)


def front(half, hidden, gain, w_pool, w_query, w_gate, pool_mix):
    tokens, width = hidden.shape
    tile = 256
    fixed = lambda a: pl.BlockSpec(a.shape, lambda i: (0,) * a.ndim)
    rowed = lambda n: pl.BlockSpec((tile, n), lambda i: (i, 0))
    gain = gain.reshape(1, width)
    outs = (w_pool.shape[1], w_query.shape[1], w_gate.shape[1])
    return pl.pallas_call(
        front_kernel,
        grid=(tokens // tile,),
        in_specs=[
            pl.BlockSpec(memory_space=pltpu.SMEM),
            rowed(width),
            fixed(gain),
            fixed(w_pool),
            fixed(w_query),
            fixed(w_gate),
            fixed(pool_mix),
        ],
        out_specs=[rowed(n) for n in outs],
        out_shape=[
            jax.ShapeDtypeStruct((tokens, outs[0]), BF16),
            jax.ShapeDtypeStruct((tokens, outs[1]), BF16),
            jax.ShapeDtypeStruct((tokens, outs[2]), BF16),
        ],
        scratch_shapes=[pltpu.VMEM((CARRY, outs[0]), BF16)],
        compiler_params=params(40),
        cost_estimate=cost(2 * tokens * width * sum(outs), 24 << 20, tokens * outs[2]),
        name="front",
    )(half, hidden, gain, w_pool, w_query, w_gate, pool_mix)


def branch_kernel(half_ref, own_ref, other_ref, w_own_ref, w_other_ref, out_ref, token_ref):
    token_ref[...] = jnp.zeros_like(token_ref)
    columns = half_columns(half_ref, out_ref.shape[1])
    own = dot(own_ref[...], w_own_ref[:, columns]).astype(BF16).astype(F32)
    other = dot(other_ref[...], w_other_ref[:, columns]).astype(BF16).astype(F32)
    out_ref[...] = (own + other).astype(BF16)


def branch(half, own, other, w_own, w_other):
    tokens, depth = own.shape
    width = w_own.shape[1]
    tile = 256
    return pl.pallas_call(
        branch_kernel,
        grid=(tokens // tile,),
        in_specs=[
            pl.BlockSpec(memory_space=pltpu.SMEM),
            pl.BlockSpec((tile, depth), lambda i: (i, 0)),
            pl.BlockSpec((tile, depth), lambda i: (i, 0)),
            pl.BlockSpec((depth, width), lambda i: (0, 0)),
            pl.BlockSpec((depth, width), lambda i: (0, 0)),
        ],
        out_specs=[
            pl.BlockSpec((tile, width // 2), lambda i: (i, 0)),
            pl.BlockSpec((8, 128), lambda i: (0, 0)),
        ],
        out_shape=[
            jax.ShapeDtypeStruct((tokens, width // 2), BF16),
            jax.ShapeDtypeStruct((8, 128), F32),
        ],
        compiler_params=params(24),
        cost_estimate=cost(2 * tokens * depth * width, 8 << 20),
        name="branch",
    )(half, own, other, w_own, w_other)


def attend_kernel(
    ids_ref, sharp_ref, query_hbm, kv_ref, _, out_ref,
    held, query_ref, scores_ref, weights_ref, sems, *, count
):
    reads, blocks = ids_ref.shape
    heads = sharp_ref.shape[0]
    length, half = held.shape[1], held.shape[2] // 2
    dim = half // heads
    block = query_ref.shape[0] // blocks
    copies = [
        pltpu.make_async_copy(
            kv_ref.at[owner_of(ids_ref[at % reads, at // reads], count)], held.at[at], sems.at[at]
        )
        for at in range(reads * blocks)
    ]

    def memory(b, at):
        rows = held[b * reads : (b + 1) * reads, :, at : at + dim]
        return rows.reshape(reads * length, dim)

    first = pltpu.make_async_copy(query_hbm, query_ref, sems.at[reads * blocks])
    first.start()
    for copy in copies:
        copy.start()
    first.wait()
    for b in range(blocks):
        for copy in copies[b * reads : (b + 1) * reads]:
            copy.wait()
        for h in range(heads):
            query = query_ref[b * block : (b + 1) * block, h * dim : (h + 1) * dim]
            scores_ref[b * heads + h] = lax.dot_general(
                memory(b, h * dim), query, (((1,), (1,)), ((), ())), preferred_element_type=F32
            )

    def soften(b, _):
        for h in range(heads):
            scores = scores_ref[b * heads + h] * (sharp_ref[h] / math.sqrt(dim))
            scores = jnp.exp(scores - jnp.max(scores, axis=0, keepdims=True))
            weights = scores * (1.0 / jnp.sum(scores, axis=0, keepdims=True))
            weights_ref[b * heads + h] = weights.astype(BF16)
        return 0

    lax.fori_loop(0, blocks, soften, 0)
    for b in range(blocks):
        for h in range(heads):
            read = lax.dot_general(
                weights_ref[b * heads + h], memory(b, half + h * dim), (((0,), (0,)), ((), ())),
                preferred_element_type=F32,
            )
            out_ref[b * block : (b + 1) * block, h * dim : (h + 1) * dim] = read.astype(BF16)


def attend(ids, sharpness, query, kv, behind, count):
    reads, blocks = ids.shape
    shape = (blocks * sharpness.shape[0], reads * kv.shape[1], query.shape[0] // blocks)
    return pl.pallas_call(
        functools.partial(attend_kernel, count=count),
        in_specs=[
            pl.BlockSpec(memory_space=pltpu.SMEM),
            pl.BlockSpec(memory_space=pltpu.SMEM),
            pl.BlockSpec(memory_space=pl.ANY),
            pl.BlockSpec(memory_space=pl.ANY),
            pl.BlockSpec(memory_space=pl.ANY),
        ],
        out_specs=pl.BlockSpec(memory_space=pltpu.VMEM),
        out_shape=jax.ShapeDtypeStruct(query.shape, BF16),
        scratch_shapes=[
            pltpu.VMEM((ids.size,) + kv.shape[1:], BF16),
            pltpu.VMEM(query.shape, BF16),
            pltpu.VMEM(shape, F32),
            pltpu.VMEM(shape, BF16),
            pltpu.SemaphoreType.DMA((ids.size + 1,)),
        ],
        compiler_params=params(16),
        cost_estimate=cost(1 << 30, 3 << 20, 1 << 19),
        name="attend",
    )(ids, sharpness, query, kv, behind)


def half_columns(half_ref, width):
    return pl.ds(pl.multiple_of(half_ref[0] * width, width), width)


def mixed_kernel(
    half_ref, own_ref, other_ref, w_own_ref, w_other_ref, pool_ref, gate_ref, out_ref, done, sems
):
    tile = own_ref.shape[0] // sems.shape[0]
    columns = half_columns(half_ref, done.shape[1])
    w_own, w_other = w_own_ref[:, columns], w_other_ref[:, columns]
    copies = []
    for i in range(sems.shape[0]):
        rows = slice(i * tile, (i + 1) * tile)
        own = dot(own_ref[rows], w_own).astype(BF16).astype(F32)
        read = own + dot(other_ref[rows], w_other).astype(BF16).astype(F32)
        done[rows] = (pool_ref[rows].astype(F32) + gate_ref[rows].astype(F32) * read).astype(BF16)
        part = pl.ds(i * tile, tile)
        copies.append(pltpu.make_async_copy(done.at[part], out_ref.at[part], sems.at[i]))
        copies[-1].start()
    for copy in copies:
        copy.wait()


def mix(half, own, other, w_own, w_other, pool, gate):
    tokens, depth = own.shape
    width = gate.shape[1]
    return pl.pallas_call(
        mixed_kernel,
        in_specs=[pl.BlockSpec(memory_space=pltpu.SMEM)]
        + [pl.BlockSpec(memory_space=pltpu.VMEM)] * 6,
        out_specs=pl.BlockSpec(memory_space=pl.ANY),
        out_shape=jax.ShapeDtypeStruct((tokens, width), BF16),
        scratch_shapes=[pltpu.VMEM((tokens, width), BF16), pltpu.SemaphoreType.DMA((4,))],
        compiler_params=params(24),
        cost_estimate=cost(4 * tokens * depth * width, 12 << 20),
        name="mixed",
    )(half, own, other, w_own, w_other, pool, gate)


def body(
    hidden, norm_gain, store, store_gain, passage_ids, w_pool, pool_mix, w_branch,
    w_query, w_key, w_value, sharpness, w_out, w_gate,
):
    half = lax.axis_index("tp").reshape(1)
    swapped = lambda a: lax.ppermute(a, "tp", SWAP)
    across = lambda a: lax.all_to_all(a, "st", split_axis=0, concat_axis=0, tiled=True)
    count = store.shape[0]
    ids = passage_ids.T
    asked = across(requests(ids, count, lax.axis_size("st")))
    offered = offer(asked, store, store_gain, w_key, w_value)
    kv = across(offered)
    w_branch, w_out, offered = lax.optimization_barrier((w_branch, w_out, offered))
    branch_other, out_other = swapped(w_branch), swapped(w_out)
    pool_out, query, gate = front(half, hidden, norm_gain, w_pool, w_query, w_gate, pool_mix)
    pool, token = branch(half, pool_out, swapped(pool_out), w_branch, branch_other)
    read = attend(ids, sharpness, query, kv, token, count)
    return mix(half, read, swapped(read), w_out, out_other, pool, gate)


def solution(mesh):
    placed = (
        P("st", None), P(), P("st", None, None), P(), P("st", None), P(None, "tp"),
        P("tp", None, None), P("tp", None), P(None, "tp"), P(None, "tp"), P(None, "tp"),
        P("tp"), P("tp", None), P(None, "tp"),
    )
    return jax.shard_map(body, mesh=mesh, in_specs=placed, out_specs=P("st", "tp"), check_vma=False)
```

```python
import functools
import math

import jax
import jax.numpy as jnp
from jax import lax
from jax.experimental import pallas as pl
from jax.experimental.pallas import tpu as pltpu
from jax.sharding import PartitionSpec as P

F32, BF16 = jnp.float32, jnp.bfloat16
EPS = 1e-05
CARRY = 16
STRIP = 32
TOGETHER = 2
SWAP = [(0, 1), (1, 0)]


def rms_norm(wide, gain):
    scale = lax.rsqrt(jnp.mean(wide * wide, axis=-1, keepdims=True) + EPS)
    return (wide * scale * gain).astype(BF16)


def dot(a, b):
    return jnp.dot(a, b, preferred_element_type=F32)


def cost(flops, bytes_accessed, transcendentals=0):
    return pl.CostEstimate(
        flops=flops, bytes_accessed=bytes_accessed, transcendentals=transcendentals
    )


def params(mib, **kw):
    return pltpu.CompilerParams(vmem_limit_bytes=mib << 20, **kw)


def owner_of(p, count):
    return lax.shift_right_logical(p * (-(-(1 << 20) // count)), 20)


def request_kernel(ids_ref, out_ref, *, count):
    holder = lax.broadcasted_iota(jnp.int32, (out_ref.shape[0], out_ref.shape[2]), 0)
    row = jnp.zeros_like(holder)
    for j in range(ids_ref.shape[0]):
        for b in range(ids_ref.shape[1]):
            p = ids_ref[j, b]
            owner = owner_of(p, count)
            row = jnp.where(holder == owner, p - owner * count + 1, row)
    out_ref[...] = row.reshape(out_ref.shape)


def requests(ids, count, holders):
    return pl.pallas_call(
        functools.partial(request_kernel, count=count),
        in_specs=[pl.BlockSpec(memory_space=pltpu.SMEM)],
        out_specs=pl.BlockSpec(memory_space=pltpu.VMEM),
        out_shape=jax.ShapeDtypeStruct((holders, 1, 128), jnp.int32),
        name="requests",
    )(ids)


def offer_kernel(
    asked_hbm, store_ref, gain_hbm, key_hbm, value_hbm, out_ref,
    rows, normed, gain_ref, w_ref, held, asked_ref, sems, out_sems,
):
    count, length, width = rows.shape
    tile = normed.shape[1]
    per = tile // length
    tiles = count // per
    half = w_ref.shape[2]
    loads = [
        pltpu.make_async_copy(
            store_ref.at[pl.ds(i * per, per)], rows.at[pl.ds(i * per, per)], sems.at[i]
        )
        for i in range(tiles)
    ]
    gain = pltpu.make_async_copy(gain_hbm, gain_ref, sems.at[tiles])
    key = pltpu.make_async_copy(key_hbm, w_ref.at[0], sems.at[tiles + 1])
    value = pltpu.make_async_copy(value_hbm, w_ref.at[1], sems.at[tiles + 2])
    wanted = pltpu.make_async_copy(asked_hbm, asked_ref, sems.at[tiles + 3])
    for copy in [gain, loads[0], key, value, *loads[1:], wanted]:
        copy.start()

    def norm(i, first, last):
        for at in range(first, last, STRIP):
            row = at % length
            wide = rows[i * per + at // length, row : row + STRIP].astype(F32)
            normed[i % 2, at : at + STRIP] = rms_norm(wide, gain_ref[...])

    gain.wait()
    loads[0].wait()
    norm(0, 0, tile)
    key.wait()
    value.wait()
    for i in range(tiles):
        if i + 1 < tiles:
            loads[i + 1].wait()
        for p in range(2):
            if i + 1 < tiles:
                norm(i + 1, p * tile // 2, (p + 1) * tile // 2)
            found = dot(normed[i % 2], w_ref[p]).astype(BF16).reshape(per, length, half)
            held[i * per : (i + 1) * per, :, p * half : (p + 1) * half] = found
    wanted.wait()
    readers = out_ref.shape[0]
    asked = [asked_ref[r, 0, 0] for r in range(readers)]
    copies = [
        pltpu.make_async_copy(held.at[jnp.maximum(asked[r] - 1, 0)], out_ref.at[r], out_sems.at[r])
        for r in range(readers)
    ]
    for r in range(readers):
        pl.when(asked[r] > 0)(copies[r].start)
    for r in range(readers):
        pl.when(asked[r] > 0)(copies[r].wait)


def offer(asked, store, gain, w_key, w_value):
    count, length, width = store.shape
    readers, half, tile = asked.shape[0], w_key.shape[1], 256
    return pl.pallas_call(
        offer_kernel,
        in_specs=[pl.BlockSpec(memory_space=pltpu.HBM)] * 5,
        out_specs=pl.BlockSpec(memory_space=pl.ANY),
        out_shape=jax.ShapeDtypeStruct((readers, length, 2 * half), BF16),
        scratch_shapes=[
            pltpu.VMEM(store.shape, BF16),
            pltpu.VMEM((2, tile, width), BF16),
            pltpu.VMEM((1, width), F32),
            pltpu.VMEM((2, width, half), BF16),
            pltpu.VMEM((count, length, 2 * half), BF16),
            pltpu.SMEM(asked.shape, jnp.int32),
            pltpu.SemaphoreType.DMA((count * length // tile + 4,)),
            pltpu.SemaphoreType.DMA((readers,)),
        ],
        compiler_params=params(60),
        cost_estimate=cost(4 * count * length * width * half, 9 << 20),
        name="offer",
    )(asked, store, gain.reshape(1, width), w_key, w_value)


def front_kernel(
    hidden_ref, gain_ref, pool_ref, query_ref, gate_ref, mix_ref,
    pool_out_ref, query_out_ref, gate_out_ref, carry,
):
    step = pl.program_id(0)
    tile = hidden_ref.shape[0]
    groups, dim = mix_ref.shape[0], mix_ref.shape[1]

    @pl.when(step == 0)
    def _():
        carry[...] = jnp.zeros_like(carry)

    normed = rms_norm(hidden_ref[...].astype(F32), gain_ref[...])
    pool_in = dot(normed, pool_ref[...]).astype(BF16)
    query_out_ref[...] = dot(normed, query_ref[...]).astype(BF16)
    gate_out_ref[...] = jax.nn.sigmoid(dot(normed, gate_ref[...])).astype(BF16)
    recent = jnp.concatenate([carry[...], pool_in], axis=0)
    carry[...] = pool_in[tile - CARRY :]
    shape = (tile, tile + CARRY)
    back = (
        lax.broadcasted_iota(jnp.int32, shape, 0)
        + CARRY
        - lax.broadcasted_iota(jnp.int32, shape, 1)
    )
    position = step * tile + lax.broadcasted_iota(jnp.int32, (tile, 1), 0)
    for g in range(groups):
        window = jnp.left_shift(2, lax.axis_index("tp") * groups + g)
        band = jnp.where((back >= 0) & (back < window), 1.0, 0.0).astype(BF16)
        columns = slice(g * dim, (g + 1) * dim)
        total = dot(band, recent[:, columns])
        count = jnp.minimum(position + 1, window).astype(F32)
        pooled = (total / count - pool_in[:, columns].astype(F32)).astype(BF16)
        pool_out_ref[:, columns] = dot(pooled, mix_ref[g]).astype(BF16)


def front(hidden, gain, w_pool, w_query, w_gate, pool_mix):
    tokens, width = hidden.shape
    tile = 256
    fixed = lambda a: pl.BlockSpec(a.shape, lambda i: (0,) * a.ndim)
    rowed = lambda n: pl.BlockSpec((tile, n), lambda i: (i, 0))
    gain = gain.reshape(1, width)
    outs = (w_pool.shape[1], w_query.shape[1], w_gate.shape[1])
    return pl.pallas_call(
        front_kernel,
        grid=(tokens // tile,),
        in_specs=[
            rowed(width),
            fixed(gain),
            fixed(w_pool),
            fixed(w_query),
            fixed(w_gate),
            fixed(pool_mix),
        ],
        out_specs=[rowed(n) for n in outs],
        out_shape=[
            jax.ShapeDtypeStruct((tokens, outs[0]), BF16),
            jax.ShapeDtypeStruct((tokens, outs[1]), BF16),
            jax.ShapeDtypeStruct((tokens, outs[2]), BF16),
        ],
        scratch_shapes=[pltpu.VMEM((CARRY, outs[0]), BF16)],
        compiler_params=params(40),
        cost_estimate=cost(2 * tokens * width * sum(outs), 24 << 20, tokens * outs[2]),
        name="front",
    )(hidden, gain, w_pool, w_query, w_gate, pool_mix)


def half_columns(width):
    return pl.ds(pl.multiple_of(lax.axis_index("tp") * width, width), width)


def branch_kernel(own_ref, other_ref, w_own_ref, w_other_ref, out_ref, token_ref):
    token_ref[...] = jnp.zeros_like(token_ref)
    columns = half_columns(out_ref.shape[1])
    own = dot(own_ref[...], w_own_ref[:, columns]).astype(BF16).astype(F32)
    other = dot(other_ref[...], w_other_ref[:, columns]).astype(BF16).astype(F32)
    out_ref[...] = (own + other).astype(BF16)


def branch(own, other, w_own, w_other):
    tokens, depth = own.shape
    width = w_own.shape[1]
    tile = 256
    return pl.pallas_call(
        branch_kernel,
        grid=(tokens // tile,),
        in_specs=[
            pl.BlockSpec((tile, depth), lambda i: (i, 0)),
            pl.BlockSpec((tile, depth), lambda i: (i, 0)),
            pl.BlockSpec((depth, width), lambda i: (0, 0)),
            pl.BlockSpec((depth, width), lambda i: (0, 0)),
        ],
        out_specs=[
            pl.BlockSpec((tile, width // 2), lambda i: (i, 0)),
            pl.BlockSpec((8, 128), lambda i: (0, 0)),
        ],
        out_shape=[
            jax.ShapeDtypeStruct((tokens, width // 2), BF16),
            jax.ShapeDtypeStruct((8, 128), F32),
        ],
        compiler_params=params(24),
        cost_estimate=cost(2 * tokens * depth * width, 8 << 20),
        name="branch",
    )(own, other, w_own, w_other)


def attend_kernel(
    ids_ref, sharp_ref, query_hbm, kv_ref, _, out_ref,
    held, query_ref, scores_ref, weights_ref, sems, *, count
):
    reads, blocks = ids_ref.shape
    heads = sharp_ref.shape[0]
    length, half = held.shape[1], held.shape[2] // 2
    dim = half // heads
    block = query_ref.shape[0] // blocks
    copies = [
        pltpu.make_async_copy(
            kv_ref.at[owner_of(ids_ref[at % reads, at // reads], count)], held.at[at], sems.at[at]
        )
        for at in range(reads * blocks)
    ]

    def memory(b, at):
        rows = held[b * reads : (b + 1) * reads, :, at : at + dim]
        return rows.reshape(reads * length, dim)

    def score(b):
        for copy in copies[b * reads : (b + 1) * reads]:
            copy.wait()
        for h in range(heads):
            query = query_ref[b * block : (b + 1) * block, h * dim : (h + 1) * dim]
            scores_ref[b * heads + h] = lax.dot_general(
                memory(b, h * dim), query, (((1,), (1,)), ((), ())), preferred_element_type=F32
            )

    def soften(b):
        for h in range(heads):
            scores = scores_ref[b * heads + h] * (sharp_ref[h] / math.sqrt(dim))
            scores = jnp.exp(scores - jnp.max(scores, axis=0, keepdims=True))
            weights = scores * (1.0 / jnp.sum(scores, axis=0, keepdims=True))
            weights_ref[b * heads + h] = weights.astype(BF16)

    def read(b):
        for h in range(heads):
            found = lax.dot_general(
                weights_ref[b * heads + h], memory(b, half + h * dim), (((0,), (0,)), ((), ())),
                preferred_element_type=F32,
            )
            out_ref[b * block : (b + 1) * block, h * dim : (h + 1) * dim] = found.astype(BF16)

    first = pltpu.make_async_copy(query_hbm, query_ref, sems.at[reads * blocks])
    first.start()
    for copy in copies:
        copy.start()
    first.wait()
    rounds = blocks // TOGETHER
    for i in range(rounds + 2):
        for delay, act in enumerate((score, soften, read)):
            if 0 <= i - delay < rounds:
                for b in range(TOGETHER):
                    act((i - delay) * TOGETHER + b)


def attend(ids, sharpness, query, kv, behind, count):
    reads, blocks = ids.shape
    shape = (blocks * sharpness.shape[0], reads * kv.shape[1], query.shape[0] // blocks)
    return pl.pallas_call(
        functools.partial(attend_kernel, count=count),
        in_specs=[
            pl.BlockSpec(memory_space=pltpu.SMEM),
            pl.BlockSpec(memory_space=pltpu.SMEM),
            pl.BlockSpec(memory_space=pltpu.HBM),
            pl.BlockSpec(memory_space=pltpu.HBM),
            pl.BlockSpec(memory_space=pl.ANY),
        ],
        out_specs=pl.BlockSpec(memory_space=pltpu.VMEM),
        out_shape=jax.ShapeDtypeStruct(query.shape, BF16),
        scratch_shapes=[
            pltpu.VMEM((ids.size,) + kv.shape[1:], BF16),
            pltpu.VMEM(query.shape, BF16),
            pltpu.VMEM(shape, F32),
            pltpu.VMEM(shape, BF16),
            pltpu.SemaphoreType.DMA((ids.size + 1,)),
        ],
        compiler_params=params(16),
        cost_estimate=cost(1 << 30, 3 << 20, 1 << 19),
        name="attend",
    )(ids, sharpness, query, kv, behind)


def own_kernel(
    own_ref, w_own_ref, w_other_ref, pool_ref, gate_ref, out_ref, columns_ref, sem
):
    columns = half_columns(gate_ref.shape[1])
    copy = pltpu.make_async_copy(w_other_ref.at[:, columns], columns_ref, sem)
    copy.start()
    tile = own_ref.shape[0] // 4
    for i in range(4):
        rows = slice(i * tile, (i + 1) * tile)
        own = dot(own_ref[rows], w_own_ref[:, columns]).astype(BF16).astype(F32)
        out_ref[rows] = pool_ref[rows].astype(F32) + gate_ref[rows].astype(F32) * own
    copy.wait()


def own_part(own, w_own, w_other, pool, gate):
    tokens, depth = own.shape
    width = gate.shape[1]
    vmem = pl.BlockSpec(memory_space=pltpu.VMEM)
    return pl.pallas_call(
        own_kernel,
        in_specs=[vmem, vmem, pl.BlockSpec(memory_space=pl.ANY), vmem, vmem],
        out_specs=[vmem, vmem],
        out_shape=[
            jax.ShapeDtypeStruct((tokens, width), F32),
            jax.ShapeDtypeStruct((depth, width), BF16),
        ],
        scratch_shapes=[pltpu.SemaphoreType.DMA],
        compiler_params=params(16),
        cost_estimate=cost(2 * tokens * depth * width, 12 << 20),
        name="own_part",
    )(own, w_own, w_other, pool, gate)


def mixed_kernel(other_ref, w_ref, sum_ref, gate_ref, out_ref, done, sems):
    tile = other_ref.shape[0] // sems.shape[0]
    copies = []
    for i in range(sems.shape[0]):
        rows = slice(i * tile, (i + 1) * tile)
        other = dot(other_ref[rows], w_ref[...]).astype(BF16).astype(F32)
        done[rows] = (sum_ref[rows] + gate_ref[rows].astype(F32) * other).astype(BF16)
        part = pl.ds(i * tile, tile)
        copies.append(pltpu.make_async_copy(done.at[part], out_ref.at[part], sems.at[i]))
        copies[-1].start()
    for copy in copies:
        copy.wait()


def mix(other, w_other, summed, gate):
    tokens, depth = other.shape
    width = gate.shape[1]
    return pl.pallas_call(
        mixed_kernel,
        in_specs=[pl.BlockSpec(memory_space=pltpu.VMEM)] * 4,
        out_specs=pl.BlockSpec(memory_space=pl.ANY),
        out_shape=jax.ShapeDtypeStruct((tokens, width), BF16),
        scratch_shapes=[pltpu.VMEM((tokens, width), BF16), pltpu.SemaphoreType.DMA((8,))],
        compiler_params=params(24),
        cost_estimate=cost(2 * tokens * depth * width, 12 << 20),
        name="mixed",
    )(other, w_other, summed, gate)


def body(
    hidden, norm_gain, store, store_gain, passage_ids, w_pool, pool_mix, w_branch,
    w_query, w_key, w_value, sharpness, w_out, w_gate,
):
    swapped = lambda a: lax.ppermute(a, "tp", SWAP)
    across = lambda a: lax.all_to_all(a, "st", split_axis=0, concat_axis=0, tiled=True)
    count = store.shape[0]
    ids = passage_ids.T
    asked = across(requests(ids, count, lax.axis_size("st")))
    offered = offer(asked, store, store_gain, w_key, w_value)
    kv = across(offered)
    w_branch, w_out, offered = lax.optimization_barrier((w_branch, w_out, offered))
    branch_other, out_other = swapped(w_branch), swapped(w_out)
    pool_out, query, gate = front(hidden, norm_gain, w_pool, w_query, w_gate, pool_mix)
    pool, token = branch(pool_out, swapped(pool_out), w_branch, branch_other)
    read = attend(ids, sharpness, query, kv, token, count)
    summed, columns = own_part(read, w_out, out_other, pool, gate)
    return mix(swapped(read), columns, summed, gate)


def solution(mesh):
    placed = (
        P("st", None), P(), P("st", None, None), P(), P("st", None), P(None, "tp"),
        P("tp", None, None), P("tp", None), P(None, "tp"), P(None, "tp"), P(None, "tp"),
        P("tp"), P("tp", None), P(None, "tp"),
    )
    return jax.shard_map(body, mesh=mesh, in_specs=placed, out_specs=P("st", "tp"), check_vma=False)
```

```python
import functools
import math

import jax
import jax.numpy as jnp
from jax import lax
from jax.experimental import pallas as pl
from jax.experimental.pallas import tpu as pltpu
from jax.sharding import PartitionSpec as P

F32, BF16 = jnp.float32, jnp.bfloat16
EPS = 1e-05
CARRY = 16
STRIP = 32
TOGETHER = 2
SWAP = [(0, 1), (1, 0)]


def rms_norm(wide, gain):
    scale = lax.rsqrt(jnp.mean(wide * wide, axis=-1, keepdims=True) + EPS)
    return (wide * scale * gain).astype(BF16)


def dot(a, b):
    return jnp.dot(a, b, preferred_element_type=F32)


def cost(flops, bytes_accessed, transcendentals=0):
    return pl.CostEstimate(
        flops=flops, bytes_accessed=bytes_accessed, transcendentals=transcendentals
    )


def params(mib, **kw):
    return pltpu.CompilerParams(vmem_limit_bytes=mib << 20, **kw)


def owner_of(p, count):
    return lax.shift_right_logical(p * (-(-(1 << 20) // count)), 20)


def request_kernel(ids_ref, out_ref, *, count):
    holder = lax.broadcasted_iota(jnp.int32, (out_ref.shape[0], out_ref.shape[2]), 0)
    row = jnp.zeros_like(holder)
    for j in range(ids_ref.shape[0]):
        for b in range(ids_ref.shape[1]):
            p = ids_ref[j, b]
            owner = owner_of(p, count)
            row = jnp.where(holder == owner, p - owner * count + 1, row)
    out_ref[...] = row.reshape(out_ref.shape)


def requests(ids, count, holders):
    return pl.pallas_call(
        functools.partial(request_kernel, count=count),
        in_specs=[pl.BlockSpec(memory_space=pltpu.SMEM)],
        out_specs=pl.BlockSpec(memory_space=pltpu.VMEM),
        out_shape=jax.ShapeDtypeStruct((holders, 1, 128), jnp.int32),
        name="requests",
    )(ids)


def project_kernel(
    store_ref, gain_hbm, key_hbm, value_hbm, out_ref, rows, normed, gain_ref, w_ref, sems
):
    count, length, width = rows.shape
    tile = normed.shape[1]
    per = tile // length
    tiles = count // per
    half = w_ref.shape[2]
    loads = [
        pltpu.make_async_copy(
            store_ref.at[pl.ds(i * per, per)], rows.at[pl.ds(i * per, per)], sems.at[i]
        )
        for i in range(tiles)
    ]
    gain = pltpu.make_async_copy(gain_hbm, gain_ref, sems.at[tiles])
    key = pltpu.make_async_copy(key_hbm, w_ref.at[0], sems.at[tiles + 1])
    value = pltpu.make_async_copy(value_hbm, w_ref.at[1], sems.at[tiles + 2])
    for copy in [gain, loads[0], key, value, *loads[1:]]:
        copy.start()

    def norm(i, first, last):
        for at in range(first, last, STRIP):
            row = at % length
            wide = rows[i * per + at // length, row : row + STRIP].astype(F32)
            normed[i % 2, at : at + STRIP] = rms_norm(wide, gain_ref[...])

    gain.wait()
    loads[0].wait()
    norm(0, 0, tile)
    key.wait()
    value.wait()
    for i in range(tiles):
        if i + 1 < tiles:
            loads[i + 1].wait()
        for p in range(2):
            if i + 1 < tiles:
                norm(i + 1, p * tile // 2, (p + 1) * tile // 2)
            found = dot(normed[i % 2], w_ref[p]).astype(BF16).reshape(per, length, half)
            out_ref[i * per : (i + 1) * per, :, p * half : (p + 1) * half] = found


def in_hbm(*arrays):
    return [pltpu.with_memory_space_constraint(a, pltpu.HBM) for a in arrays]


def project(store, gain, w_key, w_value):
    count, length, width = store.shape
    half, tile = w_key.shape[1], 256
    return pl.pallas_call(
        project_kernel,
        in_specs=[pl.BlockSpec(memory_space=pltpu.HBM)] * 4,
        out_specs=pl.BlockSpec(memory_space=pltpu.VMEM),
        out_shape=jax.ShapeDtypeStruct((count, length, 2 * half), BF16),
        scratch_shapes=[
            pltpu.VMEM(store.shape, BF16),
            pltpu.VMEM((2, tile, width), BF16),
            pltpu.VMEM((1, width), F32),
            pltpu.VMEM((2, width, half), BF16),
            pltpu.SemaphoreType.DMA((count * length // tile + 3,)),
        ],
        compiler_params=params(20),
        cost_estimate=cost(4 * count * length * width * half, 9 << 20),
        name="project",
    )(*in_hbm(store, gain.reshape(1, width), w_key, w_value))


def place_kernel(asked_hbm, kv_ref, out_ref, asked_ref, sem, out_sems):
    wanted = pltpu.make_async_copy(asked_hbm, asked_ref, sem)
    wanted.start()
    wanted.wait()
    readers = out_ref.shape[0]
    asked = [asked_ref[r, 0, 0] for r in range(readers)]
    copies = [
        pltpu.make_async_copy(kv_ref.at[jnp.maximum(asked[r] - 1, 0)], out_ref.at[r], out_sems.at[r])
        for r in range(readers)
    ]
    for r in range(readers):
        pl.when(asked[r] > 0)(copies[r].start)
    for r in range(readers):
        pl.when(asked[r] > 0)(copies[r].wait)


def place(asked, kv):
    readers = asked.shape[0]
    return pl.pallas_call(
        place_kernel,
        in_specs=[pl.BlockSpec(memory_space=pltpu.HBM), pl.BlockSpec(memory_space=pltpu.VMEM)],
        out_specs=pl.BlockSpec(memory_space=pl.ANY),
        out_shape=pltpu.HBM((readers,) + kv.shape[1:], BF16),
        scratch_shapes=[
            pltpu.SMEM(asked.shape, jnp.int32),
            pltpu.SemaphoreType.DMA,
            pltpu.SemaphoreType.DMA((readers,)),
        ],
        compiler_params=params(8),
        cost_estimate=cost(0, 5 << 20),
        name="place",
    )(asked, kv)


def front_kernel(
    hidden_ref, gain_ref, pool_ref, query_ref, gate_ref, mix_ref,
    pool_out_ref, query_out_ref, gate_out_ref, carry,
):
    step = pl.program_id(0)
    tile = hidden_ref.shape[0]
    groups, dim = mix_ref.shape[0], mix_ref.shape[1]

    @pl.when(step == 0)
    def _():
        carry[...] = jnp.zeros_like(carry)

    normed = rms_norm(hidden_ref[...].astype(F32), gain_ref[...])
    pool_in = dot(normed, pool_ref[...]).astype(BF16)
    query_out_ref[...] = dot(normed, query_ref[...]).astype(BF16)
    gate_out_ref[...] = jax.nn.sigmoid(dot(normed, gate_ref[...])).astype(BF16)
    recent = jnp.concatenate([carry[...], pool_in], axis=0)
    carry[...] = pool_in[tile - CARRY :]
    shape = (tile, tile + CARRY)
    back = (
        lax.broadcasted_iota(jnp.int32, shape, 0)
        + CARRY
        - lax.broadcasted_iota(jnp.int32, shape, 1)
    )
    position = step * tile + lax.broadcasted_iota(jnp.int32, (tile, 1), 0)
    for g in range(groups):
        window = jnp.left_shift(2, lax.axis_index("tp") * groups + g)
        band = jnp.where((back >= 0) & (back < window), 1.0, 0.0).astype(BF16)
        columns = slice(g * dim, (g + 1) * dim)
        total = dot(band, recent[:, columns])
        count = jnp.minimum(position + 1, window).astype(F32)
        pooled = (total / count - pool_in[:, columns].astype(F32)).astype(BF16)
        pool_out_ref[:, columns] = dot(pooled, mix_ref[g]).astype(BF16)


def front(hidden, gain, w_pool, w_query, w_gate, pool_mix):
    tokens, width = hidden.shape
    tile = 256
    fixed = lambda a: pl.BlockSpec(a.shape, lambda i: (0,) * a.ndim)
    rowed = lambda n: pl.BlockSpec((tile, n), lambda i: (i, 0))
    gain = gain.reshape(1, width)
    outs = (w_pool.shape[1], w_query.shape[1], w_gate.shape[1])
    return pl.pallas_call(
        front_kernel,
        grid=(tokens // tile,),
        in_specs=[
            rowed(width),
            fixed(gain),
            fixed(w_pool),
            fixed(w_query),
            fixed(w_gate),
            fixed(pool_mix),
        ],
        out_specs=[rowed(n) for n in outs],
        out_shape=[
            jax.ShapeDtypeStruct((tokens, outs[0]), BF16),
            jax.ShapeDtypeStruct((tokens, outs[1]), BF16),
            jax.ShapeDtypeStruct((tokens, outs[2]), BF16),
        ],
        scratch_shapes=[pltpu.VMEM((CARRY, outs[0]), BF16)],
        compiler_params=params(40),
        cost_estimate=cost(2 * tokens * width * sum(outs), 24 << 20, tokens * outs[2]),
        name="front",
    )(hidden, gain, w_pool, w_query, w_gate, pool_mix)


def half_columns(width):
    return pl.ds(pl.multiple_of(lax.axis_index("tp") * width, width), width)


def branch_kernel(own_ref, other_ref, w_own_ref, w_other_ref, out_ref, token_ref):
    token_ref[...] = jnp.zeros_like(token_ref)
    columns = half_columns(out_ref.shape[1])
    own = dot(own_ref[...], w_own_ref[:, columns]).astype(BF16).astype(F32)
    other = dot(other_ref[...], w_other_ref[:, columns]).astype(BF16).astype(F32)
    out_ref[...] = (own + other).astype(BF16)


def branch(own, other, w_own, w_other):
    tokens, depth = own.shape
    width = w_own.shape[1]
    tile = 256
    return pl.pallas_call(
        branch_kernel,
        grid=(tokens // tile,),
        in_specs=[
            pl.BlockSpec((tile, depth), lambda i: (i, 0)),
            pl.BlockSpec((tile, depth), lambda i: (i, 0)),
            pl.BlockSpec((depth, width), lambda i: (0, 0)),
            pl.BlockSpec((depth, width), lambda i: (0, 0)),
        ],
        out_specs=[
            pl.BlockSpec((tile, width // 2), lambda i: (i, 0)),
            pl.BlockSpec((8, 128), lambda i: (0, 0)),
        ],
        out_shape=[
            jax.ShapeDtypeStruct((tokens, width // 2), BF16),
            jax.ShapeDtypeStruct((8, 128), F32),
        ],
        compiler_params=params(24),
        cost_estimate=cost(2 * tokens * depth * width, 8 << 20),
        name="branch",
    )(own, other, w_own, w_other)


def attend_kernel(
    ids_ref, sharp_ref, query_hbm, kv_ref, _, out_ref,
    held, query_ref, scores_ref, weights_ref, sems, *, count
):
    reads, blocks = ids_ref.shape
    heads = sharp_ref.shape[0]
    length, half = held.shape[1], held.shape[2] // 2
    dim = half // heads
    block = query_ref.shape[0] // blocks
    copies = [
        pltpu.make_async_copy(
            kv_ref.at[owner_of(ids_ref[at % reads, at // reads], count)], held.at[at], sems.at[at]
        )
        for at in range(reads * blocks)
    ]

    def memory(b, at):
        rows = held[b * reads : (b + 1) * reads, :, at : at + dim]
        return rows.reshape(reads * length, dim)

    def score(b):
        for copy in copies[b * reads : (b + 1) * reads]:
            copy.wait()
        for h in range(heads):
            query = query_ref[b * block : (b + 1) * block, h * dim : (h + 1) * dim]
            scores_ref[b * heads + h] = lax.dot_general(
                memory(b, h * dim), query, (((1,), (1,)), ((), ())), preferred_element_type=F32
            )

    def soften(b):
        for h in range(heads):
            scores = scores_ref[b * heads + h] * (sharp_ref[h] / math.sqrt(dim))
            scores = jnp.exp(scores - jnp.max(scores, axis=0, keepdims=True))
            weights = scores * (1.0 / jnp.sum(scores, axis=0, keepdims=True))
            weights_ref[b * heads + h] = weights.astype(BF16)

    def read(b):
        for h in range(heads):
            found = lax.dot_general(
                weights_ref[b * heads + h], memory(b, half + h * dim), (((0,), (0,)), ((), ())),
                preferred_element_type=F32,
            )
            out_ref[b * block : (b + 1) * block, h * dim : (h + 1) * dim] = found.astype(BF16)

    first = pltpu.make_async_copy(query_hbm, query_ref, sems.at[reads * blocks])
    first.start()
    for copy in copies:
        copy.start()
    first.wait()
    rounds = blocks // TOGETHER
    for i in range(rounds + 2):
        for delay, act in enumerate((score, soften, read)):
            if 0 <= i - delay < rounds:
                for b in range(TOGETHER):
                    act((i - delay) * TOGETHER + b)


def attend(ids, sharpness, query, kv, behind, count):
    reads, blocks = ids.shape
    shape = (blocks * sharpness.shape[0], reads * kv.shape[1], query.shape[0] // blocks)
    return pl.pallas_call(
        functools.partial(attend_kernel, count=count),
        in_specs=[
            pl.BlockSpec(memory_space=pltpu.SMEM),
            pl.BlockSpec(memory_space=pltpu.SMEM),
            pl.BlockSpec(memory_space=pltpu.HBM),
            pl.BlockSpec(memory_space=pltpu.HBM),
            pl.BlockSpec(memory_space=pl.ANY),
        ],
        out_specs=pl.BlockSpec(memory_space=pltpu.VMEM),
        out_shape=jax.ShapeDtypeStruct(query.shape, BF16),
        scratch_shapes=[
            pltpu.VMEM((ids.size,) + kv.shape[1:], BF16),
            pltpu.VMEM(query.shape, BF16),
            pltpu.VMEM(shape, F32),
            pltpu.VMEM(shape, BF16),
            pltpu.SemaphoreType.DMA((ids.size + 1,)),
        ],
        compiler_params=params(16),
        cost_estimate=cost(1 << 30, 3 << 20, 1 << 19),
        name="attend",
    )(ids, sharpness, *in_hbm(query), kv, behind)


def own_kernel(
    own_ref, w_own_ref, w_other_ref, pool_ref, gate_ref, out_ref, columns_ref, sem
):
    columns = half_columns(gate_ref.shape[1])
    copy = pltpu.make_async_copy(w_other_ref.at[:, columns], columns_ref, sem)
    copy.start()
    tile = own_ref.shape[0] // 4
    for i in range(4):
        rows = slice(i * tile, (i + 1) * tile)
        own = dot(own_ref[rows], w_own_ref[:, columns]).astype(BF16).astype(F32)
        out_ref[rows] = pool_ref[rows].astype(F32) + gate_ref[rows].astype(F32) * own
    copy.wait()


def own_part(own, w_own, w_other, pool, gate):
    tokens, depth = own.shape
    width = gate.shape[1]
    vmem = pl.BlockSpec(memory_space=pltpu.VMEM)
    return pl.pallas_call(
        own_kernel,
        in_specs=[vmem, vmem, pl.BlockSpec(memory_space=pl.ANY), vmem, vmem],
        out_specs=[vmem, vmem],
        out_shape=[
            jax.ShapeDtypeStruct((tokens, width), F32),
            jax.ShapeDtypeStruct((depth, width), BF16),
        ],
        scratch_shapes=[pltpu.SemaphoreType.DMA],
        compiler_params=params(16),
        cost_estimate=cost(2 * tokens * depth * width, 12 << 20),
        name="own_part",
    )(own, w_own, w_other, pool, gate)


def mixed_kernel(other_ref, w_ref, sum_ref, gate_ref, out_ref, done, sems):
    tile = other_ref.shape[0] // sems.shape[0]
    copies = []
    for i in range(sems.shape[0]):
        rows = slice(i * tile, (i + 1) * tile)
        other = dot(other_ref[rows], w_ref[...]).astype(BF16).astype(F32)
        done[rows] = (sum_ref[rows] + gate_ref[rows].astype(F32) * other).astype(BF16)
        part = pl.ds(i * tile, tile)
        copies.append(pltpu.make_async_copy(done.at[part], out_ref.at[part], sems.at[i]))
        copies[-1].start()
    for copy in copies:
        copy.wait()


def mix(other, w_other, summed, gate):
    tokens, depth = other.shape
    width = gate.shape[1]
    return pl.pallas_call(
        mixed_kernel,
        in_specs=[pl.BlockSpec(memory_space=pltpu.VMEM)] * 4,
        out_specs=pl.BlockSpec(memory_space=pl.ANY),
        out_shape=jax.ShapeDtypeStruct((tokens, width), BF16),
        scratch_shapes=[pltpu.VMEM((tokens, width), BF16), pltpu.SemaphoreType.DMA((8,))],
        compiler_params=params(24),
        cost_estimate=cost(2 * tokens * depth * width, 12 << 20),
        name="mixed",
    )(other, w_other, summed, gate)


def body(
    hidden, norm_gain, store, store_gain, passage_ids, w_pool, pool_mix, w_branch,
    w_query, w_key, w_value, sharpness, w_out, w_gate,
):
    swapped = lambda a: lax.ppermute(a, "tp", SWAP)
    across = lambda a: lax.all_to_all(a, "st", split_axis=0, concat_axis=0, tiled=True)
    count = store.shape[0]
    ids = passage_ids.T
    asked = across(requests(ids, count, lax.axis_size("st")))
    offered = place(asked, project(store, store_gain, w_key, w_value))
    kv = across(offered)
    w_branch, w_out, offered = lax.optimization_barrier((w_branch, w_out, offered))
    branch_other, out_other = swapped(w_branch), swapped(w_out)
    pool_out, query, gate = front(hidden, norm_gain, w_pool, w_query, w_gate, pool_mix)
    pool, token = branch(pool_out, swapped(pool_out), w_branch, branch_other)
    read = attend(ids, sharpness, query, kv, token, count)
    summed, columns = own_part(read, w_out, out_other, pool, gate)
    return mix(swapped(read), columns, summed, gate)


def solution(mesh):
    placed = (
        P("st", None), P(), P("st", None, None), P(), P("st", None), P(None, "tp"),
        P("tp", None, None), P("tp", None), P(None, "tp"), P(None, "tp"), P(None, "tp"),
        P("tp"), P("tp", None), P(None, "tp"),
    )
    return jax.shard_map(body, mesh=mesh, in_specs=placed, out_specs=P("st", "tp"), check_vma=False)
```

```python
import functools
import math

import jax
import jax.numpy as jnp
from jax import lax
from jax.experimental import pallas as pl
from jax.experimental.pallas import tpu as pltpu
from jax.sharding import PartitionSpec as P

F32, BF16 = jnp.float32, jnp.bfloat16
EPS = 1e-05
CARRY = 16
STRIP = 32
TOGETHER = 2
SWAP = [(0, 1), (1, 0)]


def rms_norm(wide, gain):
    scale = lax.rsqrt(jnp.mean(wide * wide, axis=-1, keepdims=True) + EPS)
    return (wide * scale * gain).astype(BF16)


def dot(a, b):
    return jnp.dot(a, b, preferred_element_type=F32)


def cost(flops, bytes_accessed, transcendentals=0):
    return pl.CostEstimate(
        flops=flops, bytes_accessed=bytes_accessed, transcendentals=transcendentals
    )


def params(mib, **kw):
    return pltpu.CompilerParams(vmem_limit_bytes=mib << 20, **kw)


def owner_of(p, count):
    return lax.shift_right_logical(p * (-(-(1 << 20) // count)), 20)


def request_kernel(ids_ref, out_ref, *, count):
    holder = lax.broadcasted_iota(jnp.int32, (out_ref.shape[0], out_ref.shape[2]), 0)
    row = jnp.zeros_like(holder)
    for j in range(ids_ref.shape[0]):
        for b in range(ids_ref.shape[1]):
            p = ids_ref[j, b]
            owner = owner_of(p, count)
            row = jnp.where(holder == owner, p - owner * count + 1, row)
    out_ref[...] = row.reshape(out_ref.shape)


def requests(ids, count, holders):
    return pl.pallas_call(
        functools.partial(request_kernel, count=count),
        in_specs=[pl.BlockSpec(memory_space=pltpu.SMEM)],
        out_specs=pl.BlockSpec(memory_space=pltpu.VMEM),
        out_shape=jax.ShapeDtypeStruct((holders, 1, 128), jnp.int32),
        name="requests",
    )(ids)


def project_kernel(
    store_ref, gain_hbm, key_hbm, value_hbm, out_ref, rows, normed, gain_ref, w_ref, sems
):
    count, length, width = rows.shape
    tile = normed.shape[1]
    per = tile // length
    tiles = count // per
    half = w_ref.shape[2]
    loads = [
        pltpu.make_async_copy(
            store_ref.at[pl.ds(i * per, per)], rows.at[pl.ds(i * per, per)], sems.at[i]
        )
        for i in range(tiles)
    ]
    gain = pltpu.make_async_copy(gain_hbm, gain_ref, sems.at[tiles])
    key = pltpu.make_async_copy(key_hbm, w_ref.at[0], sems.at[tiles + 1])
    value = pltpu.make_async_copy(value_hbm, w_ref.at[1], sems.at[tiles + 2])
    for copy in [gain, loads[0], key, value, *loads[1:]]:
        copy.start()

    def norm(i, first, last):
        for at in range(first, last, STRIP):
            row = at % length
            wide = rows[i * per + at // length, row : row + STRIP].astype(F32)
            normed[i % 2, at : at + STRIP] = rms_norm(wide, gain_ref[...])

    gain.wait()
    loads[0].wait()
    norm(0, 0, tile)
    key.wait()
    value.wait()
    for i in range(tiles):
        if i + 1 < tiles:
            loads[i + 1].wait()
        for p in range(2):
            if i + 1 < tiles:
                norm(i + 1, p * tile // 2, (p + 1) * tile // 2)
            found = dot(normed[i % 2], w_ref[p]).astype(BF16).reshape(per, length, half)
            out_ref[i * per : (i + 1) * per, :, p * half : (p + 1) * half] = found


def in_hbm(*arrays):
    return [pltpu.with_memory_space_constraint(a, pltpu.HBM) for a in arrays]


def project(store, gain, w_key, w_value):
    count, length, width = store.shape
    half, tile = w_key.shape[1], 256
    return pl.pallas_call(
        project_kernel,
        in_specs=[pl.BlockSpec(memory_space=pltpu.HBM)] * 4,
        out_specs=pl.BlockSpec(memory_space=pltpu.VMEM),
        out_shape=jax.ShapeDtypeStruct((count, length, 2 * half), BF16),
        scratch_shapes=[
            pltpu.VMEM(store.shape, BF16),
            pltpu.VMEM((2, tile, width), BF16),
            pltpu.VMEM((1, width), F32),
            pltpu.VMEM((2, width, half), BF16),
            pltpu.SemaphoreType.DMA((count * length // tile + 3,)),
        ],
        compiler_params=params(20),
        cost_estimate=cost(4 * count * length * width * half, 9 << 20),
        name="project",
    )(*in_hbm(store, gain.reshape(1, width), w_key, w_value))


def place_kernel(asked_hbm, kv_ref, out_ref, asked_ref, sem, out_sems):
    wanted = pltpu.make_async_copy(asked_hbm, asked_ref, sem)
    wanted.start()
    wanted.wait()
    readers = out_ref.shape[0]
    asked = [asked_ref[r, 0, 0] for r in range(readers)]
    copies = [
        pltpu.make_async_copy(kv_ref.at[jnp.maximum(asked[r] - 1, 0)], out_ref.at[r], out_sems.at[r])
        for r in range(readers)
    ]
    for r in range(readers):
        pl.when(asked[r] > 0)(copies[r].start)
    for r in range(readers):
        pl.when(asked[r] > 0)(copies[r].wait)


def place(asked, kv):
    readers = asked.shape[0]
    return pl.pallas_call(
        place_kernel,
        in_specs=[pl.BlockSpec(memory_space=pltpu.HBM), pl.BlockSpec(memory_space=pltpu.VMEM)],
        out_specs=pl.BlockSpec(memory_space=pl.ANY),
        out_shape=pltpu.HBM((readers,) + kv.shape[1:], BF16),
        scratch_shapes=[
            pltpu.SMEM(asked.shape, jnp.int32),
            pltpu.SemaphoreType.DMA,
            pltpu.SemaphoreType.DMA((readers,)),
        ],
        compiler_params=params(8),
        cost_estimate=cost(0, 5 << 20),
        name="place",
    )(asked, kv)


def front_kernel(
    hidden_ref, gain_ref, pool_ref, query_ref, gate_ref, mix_ref,
    pool_out_ref, query_out_ref, gate_out_ref, carry,
):
    step = pl.program_id(0)
    tile = hidden_ref.shape[0]
    groups, dim = mix_ref.shape[0], mix_ref.shape[1]

    @pl.when(step == 0)
    def _():
        carry[...] = jnp.zeros_like(carry)

    normed = rms_norm(hidden_ref[...].astype(F32), gain_ref[...])
    pool_in = dot(normed, pool_ref[...]).astype(BF16)
    query_out_ref[...] = dot(normed, query_ref[...]).astype(BF16)
    gate_out_ref[...] = jax.nn.sigmoid(dot(normed, gate_ref[...])).astype(BF16)
    recent = jnp.concatenate([carry[...], pool_in], axis=0)
    carry[...] = pool_in[tile - CARRY :]
    shape = (tile, tile + CARRY)
    back = (
        lax.broadcasted_iota(jnp.int32, shape, 0)
        + CARRY
        - lax.broadcasted_iota(jnp.int32, shape, 1)
    )
    position = step * tile + lax.broadcasted_iota(jnp.int32, (tile, 1), 0)
    for g in range(groups):
        window = jnp.left_shift(2, lax.axis_index("tp") * groups + g)
        band = jnp.where((back >= 0) & (back < window), 1.0, 0.0).astype(BF16)
        columns = slice(g * dim, (g + 1) * dim)
        total = dot(band, recent[:, columns])
        count = jnp.minimum(position + 1, window).astype(F32)
        pooled = (total / count - pool_in[:, columns].astype(F32)).astype(BF16)
        pool_out_ref[:, columns] = dot(pooled, mix_ref[g]).astype(BF16)


def front(hidden, gain, w_pool, w_query, w_gate, pool_mix):
    tokens, width = hidden.shape
    tile = 256
    fixed = lambda a: pl.BlockSpec(a.shape, lambda i: (0,) * a.ndim)
    rowed = lambda n: pl.BlockSpec((tile, n), lambda i: (i, 0))
    gain = gain.reshape(1, width)
    outs = (w_pool.shape[1], w_query.shape[1], w_gate.shape[1])
    return pl.pallas_call(
        front_kernel,
        grid=(tokens // tile,),
        in_specs=[
            rowed(width),
            fixed(gain),
            fixed(w_pool),
            fixed(w_query),
            fixed(w_gate),
            fixed(pool_mix),
        ],
        out_specs=[rowed(n) for n in outs],
        out_shape=[
            jax.ShapeDtypeStruct((tokens, outs[0]), BF16),
            jax.ShapeDtypeStruct((tokens, outs[1]), BF16),
            jax.ShapeDtypeStruct((tokens, outs[2]), BF16),
        ],
        scratch_shapes=[pltpu.VMEM((CARRY, outs[0]), BF16)],
        compiler_params=params(40),
        cost_estimate=cost(2 * tokens * width * sum(outs), 24 << 20, tokens * outs[2]),
        name="front",
    )(hidden, gain, w_pool, w_query, w_gate, pool_mix)


def half_columns(width):
    return pl.ds(pl.multiple_of(lax.axis_index("tp") * width, width), width)


def branch_kernel(own_ref, other_ref, w_own_ref, w_other_ref, out_ref, token_ref):
    token_ref[...] = jnp.zeros_like(token_ref)
    columns = half_columns(out_ref.shape[1])
    own = dot(own_ref[...], w_own_ref[:, columns]).astype(BF16).astype(F32)
    other = dot(other_ref[...], w_other_ref[:, columns]).astype(BF16).astype(F32)
    out_ref[...] = (own + other).astype(BF16)


def branch(own, other, w_own, w_other):
    tokens, depth = own.shape
    width = w_own.shape[1]
    tile = 256
    return pl.pallas_call(
        branch_kernel,
        grid=(tokens // tile,),
        in_specs=[
            pl.BlockSpec((tile, depth), lambda i: (i, 0)),
            pl.BlockSpec((tile, depth), lambda i: (i, 0)),
            pl.BlockSpec((depth, width), lambda i: (0, 0)),
            pl.BlockSpec((depth, width), lambda i: (0, 0)),
        ],
        out_specs=[
            pl.BlockSpec((tile, width // 2), lambda i: (i, 0)),
            pl.BlockSpec((8, 128), lambda i: (0, 0)),
        ],
        out_shape=[
            jax.ShapeDtypeStruct((tokens, width // 2), BF16),
            jax.ShapeDtypeStruct((8, 128), F32),
        ],
        compiler_params=params(24),
        cost_estimate=cost(2 * tokens * depth * width, 8 << 20),
        name="branch",
    )(own, other, w_own, w_other)


def attend_kernel(
    ids_ref, sharp_ref, query_hbm, kv_ref, w_other_ref, _, out_ref, columns_ref,
    held, query_ref, scores_ref, weights_ref, sems, *, count
):
    reads, blocks = ids_ref.shape
    heads = sharp_ref.shape[0]
    length, half = held.shape[1], held.shape[2] // 2
    dim = half // heads
    block = query_ref.shape[0] // blocks
    copies = [
        pltpu.make_async_copy(
            kv_ref.at[owner_of(ids_ref[at % reads, at // reads], count)], held.at[at], sems.at[at]
        )
        for at in range(reads * blocks)
    ]

    def memory(b, at):
        rows = held[b * reads : (b + 1) * reads, :, at : at + dim]
        return rows.reshape(reads * length, dim)

    def score(b):
        for copy in copies[b * reads : (b + 1) * reads]:
            copy.wait()
        for h in range(heads):
            query = query_ref[b * block : (b + 1) * block, h * dim : (h + 1) * dim]
            scores_ref[b * heads + h] = lax.dot_general(
                memory(b, h * dim), query, (((1,), (1,)), ((), ())), preferred_element_type=F32
            )

    def soften(b):
        for h in range(heads):
            scores = scores_ref[b * heads + h] * (sharp_ref[h] / math.sqrt(dim))
            scores = jnp.exp(scores - jnp.max(scores, axis=0, keepdims=True))
            weights = scores * (1.0 / jnp.sum(scores, axis=0, keepdims=True))
            weights_ref[b * heads + h] = weights.astype(BF16)

    def read(b):
        for h in range(heads):
            found = lax.dot_general(
                weights_ref[b * heads + h], memory(b, half + h * dim), (((0,), (0,)), ((), ())),
                preferred_element_type=F32,
            )
            out_ref[b * block : (b + 1) * block, h * dim : (h + 1) * dim] = found.astype(BF16)

    first = pltpu.make_async_copy(query_hbm, query_ref, sems.at[reads * blocks])
    last = pltpu.make_async_copy(
        w_other_ref.at[:, half_columns(columns_ref.shape[1])], columns_ref,
        sems.at[reads * blocks + 1],
    )
    first.start()
    for copy in copies:
        copy.start()
    last.start()
    first.wait()
    rounds = blocks // TOGETHER
    for i in range(rounds + 2):
        for delay, act in enumerate((score, soften, read)):
            if 0 <= i - delay < rounds:
                for b in range(TOGETHER):
                    act((i - delay) * TOGETHER + b)
    last.wait()


def attend(ids, sharpness, query, kv, w_other, behind, count):
    reads, blocks = ids.shape
    shape = (blocks * sharpness.shape[0], reads * kv.shape[1], query.shape[0] // blocks)
    return pl.pallas_call(
        functools.partial(attend_kernel, count=count),
        in_specs=[
            pl.BlockSpec(memory_space=pltpu.SMEM),
            pl.BlockSpec(memory_space=pltpu.SMEM),
            pl.BlockSpec(memory_space=pltpu.HBM),
            pl.BlockSpec(memory_space=pltpu.HBM),
            pl.BlockSpec(memory_space=pltpu.HBM),
            pl.BlockSpec(memory_space=pl.ANY),
        ],
        out_specs=[pl.BlockSpec(memory_space=pltpu.VMEM)] * 2,
        out_shape=[
            pltpu.VMEM(query.shape, BF16),
            pltpu.VMEM((w_other.shape[0], w_other.shape[1] // 2), BF16),
        ],
        scratch_shapes=[
            pltpu.VMEM((ids.size,) + kv.shape[1:], BF16),
            pltpu.VMEM(query.shape, BF16),
            pltpu.VMEM(shape, F32),
            pltpu.VMEM(shape, BF16),
            pltpu.SemaphoreType.DMA((ids.size + 2,)),
        ],
        compiler_params=params(16),
        cost_estimate=cost(1 << 30, 3 << 20, 1 << 19),
        name="attend",
    )(ids, sharpness, *in_hbm(query), kv, *in_hbm(w_other), behind)


def own_kernel(own_ref, w_ref, pool_ref, gate_ref, out_ref):
    columns = half_columns(gate_ref.shape[1])
    tile = own_ref.shape[0] // 4
    for i in range(4):
        rows = slice(i * tile, (i + 1) * tile)
        own = dot(own_ref[rows], w_ref[:, columns]).astype(BF16).astype(F32)
        out_ref[rows] = pool_ref[rows].astype(F32) + gate_ref[rows].astype(F32) * own


def own_part(own, w_own, pool, gate):
    tokens, depth = own.shape
    width = gate.shape[1]
    vmem = pl.BlockSpec(memory_space=pltpu.VMEM)
    return pl.pallas_call(
        own_kernel,
        in_specs=[vmem] * 4,
        out_specs=vmem,
        out_shape=pltpu.VMEM((tokens, width), F32),
        compiler_params=params(16),
        cost_estimate=cost(2 * tokens * depth * width, 12 << 20),
        name="own_part",
    )(own, w_own, pool, gate)


def mixed_kernel(other_ref, w_ref, sum_ref, gate_ref, out_ref, done, sems):
    tile = other_ref.shape[0] // sems.shape[0]
    copies = []
    for i in range(sems.shape[0]):
        rows = slice(i * tile, (i + 1) * tile)
        other = dot(other_ref[rows], w_ref[...]).astype(BF16).astype(F32)
        done[rows] = (sum_ref[rows] + gate_ref[rows].astype(F32) * other).astype(BF16)
        part = pl.ds(i * tile, tile)
        copies.append(pltpu.make_async_copy(done.at[part], out_ref.at[part], sems.at[i]))
        copies[-1].start()
    for copy in copies:
        copy.wait()


def mix(other, w_other, summed, gate):
    tokens, depth = other.shape
    width = gate.shape[1]
    return pl.pallas_call(
        mixed_kernel,
        in_specs=[pl.BlockSpec(memory_space=pltpu.VMEM)] * 4,
        out_specs=pl.BlockSpec(memory_space=pl.ANY),
        out_shape=jax.ShapeDtypeStruct((tokens, width), BF16),
        scratch_shapes=[pltpu.VMEM((tokens, width), BF16), pltpu.SemaphoreType.DMA((8,))],
        compiler_params=params(24),
        cost_estimate=cost(2 * tokens * depth * width, 12 << 20),
        name="mixed",
    )(other, w_other, summed, gate)


def body(
    hidden, norm_gain, store, store_gain, passage_ids, w_pool, pool_mix, w_branch,
    w_query, w_key, w_value, sharpness, w_out, w_gate,
):
    swapped = lambda a: lax.ppermute(a, "tp", SWAP)
    across = lambda a: lax.all_to_all(a, "st", split_axis=0, concat_axis=0, tiled=True)
    count = store.shape[0]
    ids = passage_ids.T
    asked = across(requests(ids, count, lax.axis_size("st")))
    offered = place(asked, project(store, store_gain, w_key, w_value))
    kv = across(offered)
    w_branch, w_out, offered = lax.optimization_barrier((w_branch, w_out, offered))
    branch_other, out_other = swapped(w_branch), swapped(w_out)
    pool_out, query, gate = front(hidden, norm_gain, w_pool, w_query, w_gate, pool_mix)
    pool, token = branch(pool_out, swapped(pool_out), w_branch, branch_other)
    read, columns = attend(ids, sharpness, query, kv, out_other, token, count)
    summed = own_part(read, w_out, pool, gate)
    return mix(swapped(read), columns, summed, gate)


def solution(mesh):
    placed = (
        P("st", None), P(), P("st", None, None), P(), P("st", None), P(None, "tp"),
        P("tp", None, None), P("tp", None), P(None, "tp"), P(None, "tp"), P(None, "tp"),
        P("tp"), P("tp", None), P(None, "tp"),
    )
    return jax.shard_map(body, mesh=mesh, in_specs=placed, out_specs=P("st", "tp"), check_vma=False)
```

```python
import functools
import math

import jax
import jax.numpy as jnp
from jax import lax
from jax.experimental import pallas as pl
from jax.experimental.pallas import tpu as pltpu
from jax.sharding import PartitionSpec as P

F32, BF16 = jnp.float32, jnp.bfloat16
EPS = 1e-05
CARRY = 16
STRIP = 64
TOGETHER = 1
SWAP = [(0, 1), (1, 0)]


def rms_norm(wide, gain):
    scale = lax.rsqrt(jnp.mean(wide * wide, axis=-1, keepdims=True) + EPS)
    return (wide * scale * gain).astype(BF16)


def dot(a, b):
    return jnp.dot(a, b, preferred_element_type=F32)


def cost(flops, bytes_accessed, transcendentals=0):
    return pl.CostEstimate(
        flops=flops, bytes_accessed=bytes_accessed, transcendentals=transcendentals
    )


def params(mib, **kw):
    return pltpu.CompilerParams(vmem_limit_bytes=mib << 20, **kw)


def owner_of(p, count):
    return lax.shift_right_logical(p * (-(-(1 << 20) // count)), 20)


def request_kernel(ids_ref, out_ref, *, count):
    holder = lax.broadcasted_iota(jnp.int32, (out_ref.shape[0], out_ref.shape[2]), 0)
    row = jnp.zeros_like(holder)
    for j in range(ids_ref.shape[0]):
        for b in range(ids_ref.shape[1]):
            p = ids_ref[j, b]
            owner = owner_of(p, count)
            row = jnp.where(holder == owner, p - owner * count + 1, row)
    out_ref[...] = row.reshape(out_ref.shape)


def requests(ids, count, holders):
    return pl.pallas_call(
        functools.partial(request_kernel, count=count),
        in_specs=[pl.BlockSpec(memory_space=pltpu.SMEM)],
        out_specs=pl.BlockSpec(memory_space=pltpu.VMEM),
        out_shape=jax.ShapeDtypeStruct((holders, 1, 128), jnp.int32),
        name="requests",
    )(ids)


def project_kernel(
    store_ref, gain_hbm, key_hbm, value_hbm, out_ref, rows, normed, gain_ref, w_ref, sems
):
    count, length, width = rows.shape
    tile = normed.shape[1]
    per = tile // length
    tiles = count // per
    half = w_ref.shape[2]
    loads = [
        pltpu.make_async_copy(
            store_ref.at[pl.ds(i * per, per)], rows.at[pl.ds(i * per, per)], sems.at[i]
        )
        for i in range(tiles)
    ]
    gain = pltpu.make_async_copy(gain_hbm, gain_ref, sems.at[tiles])
    key = pltpu.make_async_copy(key_hbm, w_ref.at[0], sems.at[tiles + 1])
    value = pltpu.make_async_copy(value_hbm, w_ref.at[1], sems.at[tiles + 2])
    for copy in [gain, loads[0], key, value, *loads[1:]]:
        copy.start()

    def norm(i, first, last):
        for at in range(first, last, STRIP):
            row = at % length
            wide = rows[i * per + at // length, row : row + STRIP].astype(F32)
            normed[i % 2, at : at + STRIP] = rms_norm(wide, gain_ref[...])

    gain.wait()
    loads[0].wait()
    norm(0, 0, tile)
    key.wait()
    value.wait()
    for i in range(tiles):
        if i + 1 < tiles:
            loads[i + 1].wait()
        for p in range(2):
            if i + 1 < tiles:
                norm(i + 1, p * tile // 2, (p + 1) * tile // 2)
            found = dot(normed[i % 2], w_ref[p]).astype(BF16).reshape(per, length, half)
            out_ref[i * per : (i + 1) * per, :, p * half : (p + 1) * half] = found


def in_hbm(*arrays):
    return [pltpu.with_memory_space_constraint(a, pltpu.HBM) for a in arrays]


def project(store, gain, w_key, w_value):
    count, length, width = store.shape
    half, tile = w_key.shape[1], 256
    return pl.pallas_call(
        project_kernel,
        in_specs=[pl.BlockSpec(memory_space=pltpu.HBM)] * 4,
        out_specs=pl.BlockSpec(memory_space=pltpu.VMEM),
        out_shape=jax.ShapeDtypeStruct((count, length, 2 * half), BF16),
        scratch_shapes=[
            pltpu.VMEM(store.shape, BF16),
            pltpu.VMEM((2, tile, width), BF16),
            pltpu.VMEM((1, width), F32),
            pltpu.VMEM((2, width, half), BF16),
            pltpu.SemaphoreType.DMA((count * length // tile + 3,)),
        ],
        compiler_params=params(20),
        cost_estimate=cost(4 * count * length * width * half, 9 << 20),
        name="project",
    )(*in_hbm(store, gain.reshape(1, width), w_key, w_value))


def place_kernel(asked_hbm, kv_ref, out_ref, asked_ref, sem, out_sems):
    wanted = pltpu.make_async_copy(asked_hbm, asked_ref, sem)
    wanted.start()
    wanted.wait()
    readers = out_ref.shape[0]
    asked = [asked_ref[r, 0, 0] for r in range(readers)]
    copies = [
        pltpu.make_async_copy(kv_ref.at[jnp.maximum(asked[r] - 1, 0)], out_ref.at[r], out_sems.at[r])
        for r in range(readers)
    ]
    for r in range(readers):
        pl.when(asked[r] > 0)(copies[r].start)
    for r in range(readers):
        pl.when(asked[r] > 0)(copies[r].wait)


def place(asked, kv):
    readers = asked.shape[0]
    return pl.pallas_call(
        place_kernel,
        in_specs=[pl.BlockSpec(memory_space=pltpu.HBM), pl.BlockSpec(memory_space=pltpu.VMEM)],
        out_specs=pl.BlockSpec(memory_space=pl.ANY),
        out_shape=pltpu.HBM((readers,) + kv.shape[1:], BF16),
        scratch_shapes=[
            pltpu.SMEM(asked.shape, jnp.int32),
            pltpu.SemaphoreType.DMA,
            pltpu.SemaphoreType.DMA((readers,)),
        ],
        compiler_params=params(8),
        cost_estimate=cost(0, 5 << 20),
        name="place",
    )(asked, kv)


def front_kernel(
    hidden_ref, gain_ref, pool_ref, query_ref, gate_ref, mix_ref,
    pool_out_ref, query_out_ref, gate_out_ref, carry,
):
    step = pl.program_id(0)
    tile = hidden_ref.shape[0]
    groups, dim = mix_ref.shape[0], mix_ref.shape[1]

    @pl.when(step == 0)
    def _():
        carry[...] = jnp.zeros_like(carry)

    normed = rms_norm(hidden_ref[...].astype(F32), gain_ref[...])
    pool_in = dot(normed, pool_ref[...]).astype(BF16)
    query_out_ref[...] = dot(normed, query_ref[...]).astype(BF16)
    gate_out_ref[...] = jax.nn.sigmoid(dot(normed, gate_ref[...])).astype(BF16)
    recent = jnp.concatenate([carry[...], pool_in], axis=0)
    carry[...] = pool_in[tile - CARRY :]
    shape = (tile, tile + CARRY)
    back = (
        lax.broadcasted_iota(jnp.int32, shape, 0)
        + CARRY
        - lax.broadcasted_iota(jnp.int32, shape, 1)
    )
    position = step * tile + lax.broadcasted_iota(jnp.int32, (tile, 1), 0)
    for g in range(groups):
        window = jnp.left_shift(2, lax.axis_index("tp") * groups + g)
        band = jnp.where((back >= 0) & (back < window), 1.0, 0.0).astype(BF16)
        columns = slice(g * dim, (g + 1) * dim)
        total = dot(band, recent[:, columns])
        count = jnp.minimum(position + 1, window).astype(F32)
        pooled = (total / count - pool_in[:, columns].astype(F32)).astype(BF16)
        pool_out_ref[:, columns] = dot(pooled, mix_ref[g]).astype(BF16)


def front(hidden, gain, w_pool, w_query, w_gate, pool_mix):
    tokens, width = hidden.shape
    tile = 256
    fixed = lambda a: pl.BlockSpec(a.shape, lambda i: (0,) * a.ndim)
    rowed = lambda n: pl.BlockSpec((tile, n), lambda i: (i, 0))
    gain = gain.reshape(1, width)
    outs = (w_pool.shape[1], w_query.shape[1], w_gate.shape[1])
    return pl.pallas_call(
        front_kernel,
        grid=(tokens // tile,),
        in_specs=[
            rowed(width),
            fixed(gain),
            fixed(w_pool),
            fixed(w_query),
            fixed(w_gate),
            fixed(pool_mix),
        ],
        out_specs=[rowed(n) for n in outs],
        out_shape=[
            jax.ShapeDtypeStruct((tokens, outs[0]), BF16),
            jax.ShapeDtypeStruct((tokens, outs[1]), BF16),
            jax.ShapeDtypeStruct((tokens, outs[2]), BF16),
        ],
        scratch_shapes=[pltpu.VMEM((CARRY, outs[0]), BF16)],
        compiler_params=params(40),
        cost_estimate=cost(2 * tokens * width * sum(outs), 24 << 20, tokens * outs[2]),
        name="front",
    )(hidden, gain, w_pool, w_query, w_gate, pool_mix)


def half_columns(width):
    return pl.ds(pl.multiple_of(lax.axis_index("tp") * width, width), width)


def branch_kernel(own_ref, other_ref, w_own_ref, w_other_ref, out_ref, token_ref):
    token_ref[...] = jnp.zeros_like(token_ref)
    columns = half_columns(out_ref.shape[1])
    own = dot(own_ref[...], w_own_ref[:, columns]).astype(BF16).astype(F32)
    other = dot(other_ref[...], w_other_ref[:, columns]).astype(BF16).astype(F32)
    out_ref[...] = (own + other).astype(BF16)


def branch(own, other, w_own, w_other):
    tokens, depth = own.shape
    width = w_own.shape[1]
    tile = 256
    return pl.pallas_call(
        branch_kernel,
        grid=(tokens // tile,),
        in_specs=[
            pl.BlockSpec((tile, depth), lambda i: (i, 0)),
            pl.BlockSpec((tile, depth), lambda i: (i, 0)),
            pl.BlockSpec((depth, width), lambda i: (0, 0)),
            pl.BlockSpec((depth, width), lambda i: (0, 0)),
        ],
        out_specs=[
            pl.BlockSpec((tile, width // 2), lambda i: (i, 0)),
            pl.BlockSpec((8, 128), lambda i: (0, 0)),
        ],
        out_shape=[
            jax.ShapeDtypeStruct((tokens, width // 2), BF16),
            jax.ShapeDtypeStruct((8, 128), F32),
        ],
        compiler_params=params(24),
        cost_estimate=cost(2 * tokens * depth * width, 8 << 20),
        name="branch",
    )(own, other, w_own, w_other)


def attend_kernel(
    ids_ref, sharp_ref, query_hbm, kv_ref, w_other_ref, _, out_ref, columns_ref,
    held, query_ref, scores_ref, weights_ref, sems, *, count
):
    reads, blocks = ids_ref.shape
    heads = sharp_ref.shape[0]
    length, half = held.shape[1], held.shape[2] // 2
    dim = half // heads
    block = query_ref.shape[0] // blocks
    copies = [
        pltpu.make_async_copy(
            kv_ref.at[owner_of(ids_ref[at % reads, at // reads], count)], held.at[at], sems.at[at]
        )
        for at in range(reads * blocks)
    ]

    def memory(b, at):
        rows = held[b * reads : (b + 1) * reads, :, at : at + dim]
        return rows.reshape(reads * length, dim)

    def score(b):
        for copy in copies[b * reads : (b + 1) * reads]:
            copy.wait()
        for h in range(heads):
            query = query_ref[b * block : (b + 1) * block, h * dim : (h + 1) * dim]
            scores_ref[b * heads + h] = lax.dot_general(
                memory(b, h * dim), query, (((1,), (1,)), ((), ())), preferred_element_type=F32
            )

    def soften(b):
        for h in range(heads):
            scores = scores_ref[b * heads + h] * (sharp_ref[h] / math.sqrt(dim))
            scores = jnp.exp(scores - jnp.max(scores, axis=0, keepdims=True))
            weights = scores * (1.0 / jnp.sum(scores, axis=0, keepdims=True))
            weights_ref[b * heads + h] = weights.astype(BF16)

    def read(b):
        for h in range(heads):
            found = lax.dot_general(
                weights_ref[b * heads + h], memory(b, half + h * dim), (((0,), (0,)), ((), ())),
                preferred_element_type=F32,
            )
            out_ref[b * block : (b + 1) * block, h * dim : (h + 1) * dim] = found.astype(BF16)

    first = pltpu.make_async_copy(query_hbm, query_ref, sems.at[reads * blocks])
    last = pltpu.make_async_copy(
        w_other_ref.at[:, half_columns(columns_ref.shape[1])], columns_ref,
        sems.at[reads * blocks + 1],
    )
    first.start()
    for copy in copies:
        copy.start()
    last.start()
    first.wait()
    rounds = blocks // TOGETHER
    for i in range(rounds + 2):
        for delay, act in enumerate((score, soften, read)):
            if 0 <= i - delay < rounds:
                for b in range(TOGETHER):
                    act((i - delay) * TOGETHER + b)
    last.wait()


def attend(ids, sharpness, query, kv, w_other, behind, count):
    reads, blocks = ids.shape
    shape = (blocks * sharpness.shape[0], reads * kv.shape[1], query.shape[0] // blocks)
    return pl.pallas_call(
        functools.partial(attend_kernel, count=count),
        in_specs=[
            pl.BlockSpec(memory_space=pltpu.SMEM),
            pl.BlockSpec(memory_space=pltpu.SMEM),
            pl.BlockSpec(memory_space=pltpu.HBM),
            pl.BlockSpec(memory_space=pltpu.HBM),
            pl.BlockSpec(memory_space=pltpu.HBM),
            pl.BlockSpec(memory_space=pl.ANY),
        ],
        out_specs=[pl.BlockSpec(memory_space=pltpu.VMEM)] * 2,
        out_shape=[
            pltpu.VMEM(query.shape, BF16),
            pltpu.VMEM((w_other.shape[0], w_other.shape[1] // 2), BF16),
        ],
        scratch_shapes=[
            pltpu.VMEM((ids.size,) + kv.shape[1:], BF16),
            pltpu.VMEM(query.shape, BF16),
            pltpu.VMEM(shape, F32),
            pltpu.VMEM(shape, BF16),
            pltpu.SemaphoreType.DMA((ids.size + 2,)),
        ],
        compiler_params=params(16),
        cost_estimate=cost(1 << 30, 3 << 20, 1 << 19),
        name="attend",
    )(ids, sharpness, *in_hbm(query), kv, *in_hbm(w_other), behind)


def own_kernel(own_ref, w_ref, pool_ref, gate_ref, out_ref):
    columns = half_columns(gate_ref.shape[1])
    tile = own_ref.shape[0] // 4
    for i in range(4):
        rows = slice(i * tile, (i + 1) * tile)
        own = dot(own_ref[rows], w_ref[:, columns]).astype(BF16).astype(F32)
        out_ref[rows] = pool_ref[rows].astype(F32) + gate_ref[rows].astype(F32) * own


def own_part(own, w_own, pool, gate):
    tokens, depth = own.shape
    width = gate.shape[1]
    vmem = pl.BlockSpec(memory_space=pltpu.VMEM)
    return pl.pallas_call(
        own_kernel,
        in_specs=[vmem] * 4,
        out_specs=vmem,
        out_shape=pltpu.VMEM((tokens, width), F32),
        compiler_params=params(16),
        cost_estimate=cost(2 * tokens * depth * width, 12 << 20),
        name="own_part",
    )(own, w_own, pool, gate)


def mixed_kernel(other_ref, w_ref, sum_ref, gate_ref, out_ref, done, sems):
    tile = other_ref.shape[0] // sems.shape[0]
    copies = []
    for i in range(sems.shape[0]):
        rows = slice(i * tile, (i + 1) * tile)
        other = dot(other_ref[rows], w_ref[...]).astype(BF16).astype(F32)
        done[rows] = (sum_ref[rows] + gate_ref[rows].astype(F32) * other).astype(BF16)
        part = pl.ds(i * tile, tile)
        copies.append(pltpu.make_async_copy(done.at[part], out_ref.at[part], sems.at[i]))
        copies[-1].start()
    for copy in copies:
        copy.wait()


def mix(other, w_other, summed, gate):
    tokens, depth = other.shape
    width = gate.shape[1]
    return pl.pallas_call(
        mixed_kernel,
        in_specs=[pl.BlockSpec(memory_space=pltpu.VMEM)] * 4,
        out_specs=pl.BlockSpec(memory_space=pl.ANY),
        out_shape=jax.ShapeDtypeStruct((tokens, width), BF16),
        scratch_shapes=[pltpu.VMEM((tokens, width), BF16), pltpu.SemaphoreType.DMA((4,))],
        compiler_params=params(24),
        cost_estimate=cost(2 * tokens * depth * width, 12 << 20),
        name="mixed",
    )(other, w_other, summed, gate)


def body(
    hidden, norm_gain, store, store_gain, passage_ids, w_pool, pool_mix, w_branch,
    w_query, w_key, w_value, sharpness, w_out, w_gate,
):
    swapped = lambda a: lax.ppermute(a, "tp", SWAP)
    across = lambda a: lax.all_to_all(a, "st", split_axis=0, concat_axis=0, tiled=True)
    count = store.shape[0]
    ids = passage_ids.T
    asked = across(requests(ids, count, lax.axis_size("st")))
    offered = place(asked, project(store, store_gain, w_key, w_value))
    kv = across(offered)
    w_branch, w_out, offered = lax.optimization_barrier((w_branch, w_out, offered))
    branch_other, out_other = swapped(w_branch), swapped(w_out)
    pool_out, query, gate = front(hidden, norm_gain, w_pool, w_query, w_gate, pool_mix)
    pool, token = branch(pool_out, swapped(pool_out), w_branch, branch_other)
    read, columns = attend(ids, sharpness, query, kv, out_other, token, count)
    summed = own_part(read, w_out, pool, gate)
    return mix(swapped(read), columns, summed, gate)


def solution(mesh):
    placed = (
        P("st", None), P(), P("st", None, None), P(), P("st", None), P(None, "tp"),
        P("tp", None, None), P("tp", None), P(None, "tp"), P(None, "tp"), P(None, "tp"),
        P("tp"), P("tp", None), P(None, "tp"),
    )
    return jax.shard_map(body, mesh=mesh, in_specs=placed, out_specs=P("st", "tp"), check_vma=False)
```

```python
import functools
import math

import jax
import jax.numpy as jnp
from jax import lax
from jax.experimental import pallas as pl
from jax.experimental.pallas import tpu as pltpu
from jax.sharding import PartitionSpec as P

F32, BF16 = jnp.float32, jnp.bfloat16
EPS = 1e-05
CARRY = 16
STRIP = 64
TOGETHER = 1
SWAP = [(0, 1), (1, 0)]


def rms_norm(wide, gain):
    scale = lax.rsqrt(jnp.mean(wide * wide, axis=-1, keepdims=True) + EPS)
    return (wide * scale * gain).astype(BF16)


def dot(a, b):
    return jnp.dot(a, b, preferred_element_type=F32)


def cost(flops, bytes_accessed, transcendentals=0):
    return pl.CostEstimate(
        flops=flops, bytes_accessed=bytes_accessed, transcendentals=transcendentals
    )


def params(mib, **kw):
    return pltpu.CompilerParams(vmem_limit_bytes=mib << 20, **kw)


def owner_of(p, count):
    return lax.shift_right_logical(p * (-(-(1 << 20) // count)), 20)


def request_kernel(ids_ref, out_ref, *, count):
    holder = lax.broadcasted_iota(jnp.int32, (out_ref.shape[0], out_ref.shape[2]), 0)
    row = jnp.zeros_like(holder)
    for j in range(ids_ref.shape[0]):
        for b in range(ids_ref.shape[1]):
            p = ids_ref[j, b]
            owner = owner_of(p, count)
            row = jnp.where(holder == owner, p - owner * count + 1, row)
    out_ref[...] = row.reshape(out_ref.shape)


def requests(ids, count, holders):
    return pl.pallas_call(
        functools.partial(request_kernel, count=count),
        in_specs=[pl.BlockSpec(memory_space=pltpu.SMEM)],
        out_specs=pl.BlockSpec(memory_space=pltpu.VMEM),
        out_shape=jax.ShapeDtypeStruct((holders, 1, 128), jnp.int32),
        name="requests",
    )(ids)


def project_kernel(
    store_ref, gain_hbm, key_hbm, value_hbm, out_ref, rows, normed, gain_ref, w_ref, sems
):
    count, length, width = rows.shape
    tile = normed.shape[1]
    per = tile // length
    tiles = count // per
    half = w_ref.shape[2]
    loads = [
        pltpu.make_async_copy(
            store_ref.at[pl.ds(i * per, per)], rows.at[pl.ds(i * per, per)], sems.at[i]
        )
        for i in range(tiles)
    ]
    gain = pltpu.make_async_copy(gain_hbm, gain_ref, sems.at[tiles])
    key = pltpu.make_async_copy(key_hbm, w_ref.at[0], sems.at[tiles + 1])
    value = pltpu.make_async_copy(value_hbm, w_ref.at[1], sems.at[tiles + 2])
    for copy in [gain, loads[0], key, value, *loads[1:]]:
        copy.start()

    def norm(i, first, last):
        for at in range(first, last, STRIP):
            row = at % length
            wide = rows[i * per + at // length, row : row + STRIP].astype(F32)
            normed[i % 2, at : at + STRIP] = rms_norm(wide, gain_ref[...])

    gain.wait()
    loads[0].wait()
    norm(0, 0, tile)
    key.wait()
    for i in range(tiles):
        if i + 1 < tiles:
            loads[i + 1].wait()
        for p in range(2):
            if i + 1 < tiles:
                norm(i + 1, p * tile // 2, (p + 1) * tile // 2)
            if i == 0 and p == 1:
                value.wait()
            found = dot(normed[i % 2], w_ref[p]).astype(BF16).reshape(per, length, half)
            out_ref[i * per : (i + 1) * per, :, p * half : (p + 1) * half] = found


def in_hbm(*arrays):
    return [pltpu.with_memory_space_constraint(a, pltpu.HBM) for a in arrays]


def project(store, gain, w_key, w_value):
    count, length, width = store.shape
    half, tile = w_key.shape[1], 256
    return pl.pallas_call(
        project_kernel,
        in_specs=[pl.BlockSpec(memory_space=pltpu.HBM)] * 4,
        out_specs=pl.BlockSpec(memory_space=pltpu.VMEM),
        out_shape=jax.ShapeDtypeStruct((count, length, 2 * half), BF16),
        scratch_shapes=[
            pltpu.VMEM(store.shape, BF16),
            pltpu.VMEM((2, tile, width), BF16),
            pltpu.VMEM((1, width), F32),
            pltpu.VMEM((2, width, half), BF16),
            pltpu.SemaphoreType.DMA((count * length // tile + 3,)),
        ],
        compiler_params=params(20),
        cost_estimate=cost(4 * count * length * width * half, 9 << 20),
        name="project",
    )(*in_hbm(store, gain.reshape(1, width), w_key, w_value))


def place_kernel(asked_hbm, kv_ref, out_ref, asked_ref, sem, out_sems):
    wanted = pltpu.make_async_copy(asked_hbm, asked_ref, sem)
    wanted.start()
    wanted.wait()
    readers = out_ref.shape[0]
    asked = [asked_ref[r, 0, 0] for r in range(readers)]
    copies = [
        pltpu.make_async_copy(kv_ref.at[jnp.maximum(asked[r] - 1, 0)], out_ref.at[r], out_sems.at[r])
        for r in range(readers)
    ]
    for r in range(readers):
        pl.when(asked[r] > 0)(copies[r].start)
    for r in range(readers):
        pl.when(asked[r] > 0)(copies[r].wait)


def place(asked, kv):
    readers = asked.shape[0]
    return pl.pallas_call(
        place_kernel,
        in_specs=[pl.BlockSpec(memory_space=pltpu.HBM), pl.BlockSpec(memory_space=pltpu.VMEM)],
        out_specs=pl.BlockSpec(memory_space=pl.ANY),
        out_shape=pltpu.HBM((readers,) + kv.shape[1:], BF16),
        scratch_shapes=[
            pltpu.SMEM(asked.shape, jnp.int32),
            pltpu.SemaphoreType.DMA,
            pltpu.SemaphoreType.DMA((readers,)),
        ],
        compiler_params=params(8),
        cost_estimate=cost(0, 5 << 20),
        name="place",
    )(asked, kv)


def front_kernel(
    hidden_ref, gain_ref, pool_ref, query_ref, gate_ref, mix_ref,
    pool_out_ref, query_out_ref, gate_out_ref, carry,
):
    step = pl.program_id(0)
    tile = hidden_ref.shape[0]
    groups, dim = mix_ref.shape[0], mix_ref.shape[1]

    @pl.when(step == 0)
    def _():
        carry[...] = jnp.zeros_like(carry)

    normed = rms_norm(hidden_ref[...].astype(F32), gain_ref[...])
    pool_in = dot(normed, pool_ref[...]).astype(BF16)
    query_out_ref[...] = dot(normed, query_ref[...]).astype(BF16)
    gate_out_ref[...] = jax.nn.sigmoid(dot(normed, gate_ref[...])).astype(BF16)
    recent = jnp.concatenate([carry[...], pool_in], axis=0)
    carry[...] = pool_in[tile - CARRY :]
    shape = (tile, tile + CARRY)
    back = (
        lax.broadcasted_iota(jnp.int32, shape, 0)
        + CARRY
        - lax.broadcasted_iota(jnp.int32, shape, 1)
    )
    position = step * tile + lax.broadcasted_iota(jnp.int32, (tile, 1), 0)
    for g in range(groups):
        window = jnp.left_shift(2, lax.axis_index("tp") * groups + g)
        band = jnp.where((back >= 0) & (back < window), 1.0, 0.0).astype(BF16)
        columns = slice(g * dim, (g + 1) * dim)
        total = dot(band, recent[:, columns])
        count = jnp.minimum(position + 1, window).astype(F32)
        pooled = (total / count - pool_in[:, columns].astype(F32)).astype(BF16)
        pool_out_ref[:, columns] = dot(pooled, mix_ref[g]).astype(BF16)


def front(hidden, gain, w_pool, w_query, w_gate, pool_mix):
    tokens, width = hidden.shape
    tile = 256
    fixed = lambda a: pl.BlockSpec(a.shape, lambda i: (0,) * a.ndim)
    rowed = lambda n: pl.BlockSpec((tile, n), lambda i: (i, 0))
    gain = gain.reshape(1, width)
    outs = (w_pool.shape[1], w_query.shape[1], w_gate.shape[1])
    return pl.pallas_call(
        front_kernel,
        grid=(tokens // tile,),
        in_specs=[
            rowed(width),
            fixed(gain),
            fixed(w_pool),
            fixed(w_query),
            fixed(w_gate),
            fixed(pool_mix),
        ],
        out_specs=[rowed(n) for n in outs],
        out_shape=[
            jax.ShapeDtypeStruct((tokens, outs[0]), BF16),
            jax.ShapeDtypeStruct((tokens, outs[1]), BF16),
            jax.ShapeDtypeStruct((tokens, outs[2]), BF16),
        ],
        scratch_shapes=[pltpu.VMEM((CARRY, outs[0]), BF16)],
        compiler_params=params(40),
        cost_estimate=cost(2 * tokens * width * sum(outs), 24 << 20, tokens * outs[2]),
        name="front",
    )(hidden, gain, w_pool, w_query, w_gate, pool_mix)


def half_columns(width):
    return pl.ds(pl.multiple_of(lax.axis_index("tp") * width, width), width)


def branch_kernel(own_ref, other_ref, w_own_ref, w_other_ref, out_ref, token_ref):
    token_ref[...] = jnp.zeros_like(token_ref)
    columns = half_columns(out_ref.shape[1])
    own = dot(own_ref[...], w_own_ref[:, columns]).astype(BF16).astype(F32)
    other = dot(other_ref[...], w_other_ref[:, columns]).astype(BF16).astype(F32)
    out_ref[...] = (own + other).astype(BF16)


def branch(own, other, w_own, w_other):
    tokens, depth = own.shape
    width = w_own.shape[1]
    tile = 256
    return pl.pallas_call(
        branch_kernel,
        grid=(tokens // tile,),
        in_specs=[
            pl.BlockSpec((tile, depth), lambda i: (i, 0)),
            pl.BlockSpec((tile, depth), lambda i: (i, 0)),
            pl.BlockSpec((depth, width), lambda i: (0, 0)),
            pl.BlockSpec((depth, width), lambda i: (0, 0)),
        ],
        out_specs=[
            pl.BlockSpec((tile, width // 2), lambda i: (i, 0)),
            pl.BlockSpec((8, 128), lambda i: (0, 0)),
        ],
        out_shape=[
            jax.ShapeDtypeStruct((tokens, width // 2), BF16),
            jax.ShapeDtypeStruct((8, 128), F32),
        ],
        compiler_params=params(24),
        cost_estimate=cost(2 * tokens * depth * width, 8 << 20),
        name="branch",
    )(own, other, w_own, w_other)


def attend_kernel(
    ids_ref, sharp_ref, query_hbm, kv_ref, w_other_ref, _, out_ref, columns_ref,
    held, query_ref, scores_ref, weights_ref, sems, *, count
):
    reads, blocks = ids_ref.shape
    heads = sharp_ref.shape[0]
    length, half = held.shape[1], held.shape[2] // 2
    dim = half // heads
    block = query_ref.shape[0] // blocks
    copies = [
        pltpu.make_async_copy(
            kv_ref.at[owner_of(ids_ref[at % reads, at // reads], count)], held.at[at], sems.at[at]
        )
        for at in range(reads * blocks)
    ]

    def memory(b, at):
        rows = held[b * reads : (b + 1) * reads, :, at : at + dim]
        return rows.reshape(reads * length, dim)

    def score(b):
        for copy in copies[b * reads : (b + 1) * reads]:
            copy.wait()
        for h in range(heads):
            query = query_ref[b * block : (b + 1) * block, h * dim : (h + 1) * dim]
            scores_ref[b * heads + h] = lax.dot_general(
                memory(b, h * dim), query, (((1,), (1,)), ((), ())), preferred_element_type=F32
            )

    def soften(b):
        for h in range(heads):
            scores = scores_ref[b * heads + h] * (sharp_ref[h] / math.sqrt(dim))
            scores = jnp.exp(scores - jnp.max(scores, axis=0, keepdims=True))
            weights = scores * (1.0 / jnp.sum(scores, axis=0, keepdims=True))
            weights_ref[b * heads + h] = weights.astype(BF16)

    def read(b):
        for h in range(heads):
            found = lax.dot_general(
                weights_ref[b * heads + h], memory(b, half + h * dim), (((0,), (0,)), ((), ())),
                preferred_element_type=F32,
            )
            out_ref[b * block : (b + 1) * block, h * dim : (h + 1) * dim] = found.astype(BF16)

    first = pltpu.make_async_copy(query_hbm, query_ref, sems.at[reads * blocks])
    last = pltpu.make_async_copy(
        w_other_ref.at[:, half_columns(columns_ref.shape[1])], columns_ref,
        sems.at[reads * blocks + 1],
    )
    first.start()
    for copy in copies:
        copy.start()
    last.start()
    first.wait()
    rounds = blocks // TOGETHER
    for i in range(rounds + 2):
        for delay, act in enumerate((score, soften, read)):
            if 0 <= i - delay < rounds:
                for b in range(TOGETHER):
                    act((i - delay) * TOGETHER + b)
    last.wait()


def attend(ids, sharpness, query, kv, w_other, behind, count):
    reads, blocks = ids.shape
    shape = (blocks * sharpness.shape[0], reads * kv.shape[1], query.shape[0] // blocks)
    return pl.pallas_call(
        functools.partial(attend_kernel, count=count),
        in_specs=[
            pl.BlockSpec(memory_space=pltpu.SMEM),
            pl.BlockSpec(memory_space=pltpu.SMEM),
            pl.BlockSpec(memory_space=pltpu.HBM),
            pl.BlockSpec(memory_space=pltpu.HBM),
            pl.BlockSpec(memory_space=pltpu.HBM),
            pl.BlockSpec(memory_space=pl.ANY),
        ],
        out_specs=[pl.BlockSpec(memory_space=pltpu.VMEM)] * 2,
        out_shape=[
            pltpu.VMEM(query.shape, BF16),
            pltpu.VMEM((w_other.shape[0], w_other.shape[1] // 2), BF16),
        ],
        scratch_shapes=[
            pltpu.VMEM((ids.size,) + kv.shape[1:], BF16),
            pltpu.VMEM(query.shape, BF16),
            pltpu.VMEM(shape, F32),
            pltpu.VMEM(shape, BF16),
            pltpu.SemaphoreType.DMA((ids.size + 2,)),
        ],
        compiler_params=params(16),
        cost_estimate=cost(1 << 30, 3 << 20, 1 << 19),
        name="attend",
    )(ids, sharpness, *in_hbm(query), kv, *in_hbm(w_other), behind)


def own_kernel(own_ref, w_ref, pool_ref, gate_ref, out_ref):
    columns = half_columns(gate_ref.shape[1])
    tile = own_ref.shape[0] // 4
    for i in range(4):
        rows = slice(i * tile, (i + 1) * tile)
        own = dot(own_ref[rows], w_ref[:, columns]).astype(BF16).astype(F32)
        out_ref[rows] = pool_ref[rows].astype(F32) + gate_ref[rows].astype(F32) * own


def own_part(own, w_own, pool, gate):
    tokens, depth = own.shape
    width = gate.shape[1]
    vmem = pl.BlockSpec(memory_space=pltpu.VMEM)
    return pl.pallas_call(
        own_kernel,
        in_specs=[vmem] * 4,
        out_specs=vmem,
        out_shape=pltpu.VMEM((tokens, width), F32),
        compiler_params=params(16),
        cost_estimate=cost(2 * tokens * depth * width, 12 << 20),
        name="own_part",
    )(own, w_own, pool, gate)


def mixed_kernel(other_ref, w_ref, sum_ref, gate_ref, out_ref, done, sems):
    tile = other_ref.shape[0] // sems.shape[0]
    copies = []
    for i in range(sems.shape[0]):
        rows = slice(i * tile, (i + 1) * tile)
        other = dot(other_ref[rows], w_ref[...]).astype(BF16).astype(F32)
        done[rows] = (sum_ref[rows] + gate_ref[rows].astype(F32) * other).astype(BF16)
        part = pl.ds(i * tile, tile)
        copies.append(pltpu.make_async_copy(done.at[part], out_ref.at[part], sems.at[i]))
        copies[-1].start()
    for copy in copies:
        copy.wait()


def mix(other, w_other, summed, gate):
    tokens, depth = other.shape
    width = gate.shape[1]
    return pl.pallas_call(
        mixed_kernel,
        in_specs=[pl.BlockSpec(memory_space=pltpu.VMEM)] * 4,
        out_specs=pl.BlockSpec(memory_space=pl.ANY),
        out_shape=jax.ShapeDtypeStruct((tokens, width), BF16),
        scratch_shapes=[pltpu.VMEM((tokens, width), BF16), pltpu.SemaphoreType.DMA((4,))],
        compiler_params=params(24),
        cost_estimate=cost(2 * tokens * depth * width, 12 << 20),
        name="mixed",
    )(other, w_other, summed, gate)


def body(
    hidden, norm_gain, store, store_gain, passage_ids, w_pool, pool_mix, w_branch,
    w_query, w_key, w_value, sharpness, w_out, w_gate,
):
    swapped = lambda a: lax.ppermute(a, "tp", SWAP)
    across = lambda a: lax.all_to_all(a, "st", split_axis=0, concat_axis=0, tiled=True)
    count = store.shape[0]
    ids = passage_ids.T
    asked = across(requests(ids, count, lax.axis_size("st")))
    offered = place(asked, project(store, store_gain, w_key, w_value))
    kv = across(offered)
    w_branch, w_out, offered = lax.optimization_barrier((w_branch, w_out, offered))
    branch_other, out_other = swapped(w_branch), swapped(w_out)
    pool_out, query, gate = front(hidden, norm_gain, w_pool, w_query, w_gate, pool_mix)
    pool, token = branch(pool_out, swapped(pool_out), w_branch, branch_other)
    read, columns = attend(ids, sharpness, query, kv, out_other, token, count)
    summed = own_part(read, w_out, pool, gate)
    return mix(swapped(read), columns, summed, gate)


def solution(mesh):
    placed = (
        P("st", None), P(), P("st", None, None), P(), P("st", None), P(None, "tp"),
        P("tp", None, None), P("tp", None), P(None, "tp"), P(None, "tp"), P(None, "tp"),
        P("tp"), P("tp", None), P(None, "tp"),
    )
    return jax.shard_map(body, mesh=mesh, in_specs=placed, out_specs=P("st", "tp"), check_vma=False)
```
